128 devices in a mesh: rep: 2 (over z_hi), fs: 32 (over z_lo, y, x), tp: 2 (over core).
Axes of the slice: x: 4, y: 4, z: 4 (z_hi: 2, z_lo: 2; z = z_hi * 2 + z_lo), core: 2. Of those that a mesh axis runs over, the one named last changes fastest.
Arguments:
- hidden_in: bfloat16 [40960, 2048], P(('rep', 'fs'), 'tp'), may hold values from -6 to 6
- mix_gain: float32 [2048], replicated, may hold values from 0.1 to 1.9
- w_value: bfloat16 [2048, 1024], P('fs', 'tp'), may hold values from -0.125 to 0.125
- w_gate: bfloat16 [2048, 1024], P('fs', 'tp'), may hold values from -0.125 to 0.125
- conv_taps: float32 [31, 1024], P(None, 'tp'), may hold values from -5 to 5
- conv_bias: float32 [1024], P('tp'), may hold values from -3 to 3
- chan_gain: float32 [1024], P('tp'), may hold values from 0.1 to 1.9
- chan_bias: float32 [1024], P('tp'), may hold values from -3 to 3
- w_back: bfloat16 [1024, 2048], P('tp', 'fs'), may hold values from -0.1875 to 0.1875
- feed_gain: float32 [2048], replicated, may hold values from 0.1 to 1.9
- w_up: bfloat16 [2048, 8192], P(None, ('fs', 'tp')), may hold values from -0.125 to 0.125
- w_down: bfloat16 [8192, 2048], P(('fs', 'tp')), may hold values from -0.0625 to 0.0625
Outputs:
- layer_out: bfloat16 [40960, 2048], P(('rep', 'fs'), 'tp')
The draws below stay inside these ranges and needn't reach their ends.
All inputs are finite; a program needn't handle non-finite values.
Results may differ from the reference program's by a relative error of at most 0.015.
Values may be sent and summed in bfloat16 or wider, within the bound.
A program may use at most 128 MiB of HBM per device.

```python
import jax
import jax.numpy as jnp
from jax import lax

D = 2048
CH = 1024
FF = 8192
KW = 31
LEN = 128
TOKENS = 40960
N_FS = 32
N_TP = 2


def draw_conv_taps(key, part):
    entry_key, rough_key = jax.random.split(jax.random.fold_in(key, 11))
    channel_ramp = jnp.arange(CH, dtype=jnp.float32) / CH
    roughness = jax.random.uniform(rough_key, (KW, CH), jnp.float32, 0.5, 1.5)
    entries = jnp.clip(jax.random.normal(entry_key, (KW, CH), jnp.float32), -4.0, 4.0)
    growth = 3.0 ** channel_ramp
    return (entries * roughness * growth[None, :] * KW ** (-0.5)).astype(jnp.float32)


def shard_levels(own_key, dims, cuts, least, high):
    loudness, own = 1.0, jax.random.fold_in(own_key, 6)
    for dim, blocks in cuts:
        heights = jnp.exp(jax.random.uniform(jax.random.fold_in(own, dim), (blocks,), jnp.float32, least / len(cuts), high / len(cuts)))
        loudness = loudness * jnp.repeat(heights, dims[dim] // blocks).reshape([-1 if axis == dim else 1 for axis in range(len(dims))])
    return loudness


def gaussian(own_key, extent, deviation, most, cuts=(), kind=jnp.bfloat16):
    values = deviation * jax.random.normal(own_key, extent, jnp.float32)
    if cuts:
        values = values * shard_levels(own_key, extent, cuts, -0.22, 0.18)
    return jnp.clip(values, -most, most).astype(kind)


def setup_inputs(seed: int = 0) -> dict:
    key_of = jax.random.split(jax.random.key(seed), 13)
    hidden_in = gaussian(key_of[0], (TOKENS, D), 1.0, 6.0, ((0, 64), (1, 2)))
    mix_gain = jnp.clip(1.0 + 0.18 * jax.random.normal(key_of[1], (D,), jnp.float32), 0.1, 1.9)
    w_value = gaussian(key_of[2], (D, CH), D ** -0.5, 0.125, ((0, 32), (1, 2)))
    w_gate = gaussian(key_of[3], (D, CH), D ** -0.5, 0.125, ((0, 32), (1, 2)))
    conv_taps = draw_conv_taps(jax.random.fold_in(key_of[12], 71), 0)
    conv_bias = gaussian(key_of[5], (CH,), 0.5, 3.0, ((0, 2),), jnp.float32)
    chan_gain = jnp.clip(1.0 + 0.18 * jax.random.normal(key_of[6], (CH,), jnp.float32), 0.1, 1.9)
    chan_bias = gaussian(key_of[7], (CH,), 0.5, 3.0, ((0, 2),), jnp.float32)
    w_back = gaussian(key_of[8], (CH, D), CH ** -0.5, 0.1875, ((0, 2), (1, 32)))
    feed_gain = jnp.clip(1.0 + 0.18 * jax.random.normal(key_of[9], (D,), jnp.float32), 0.1, 1.9)
    w_up = gaussian(key_of[10], (D, FF), D ** -0.5, 0.125, ((1, 64),))
    w_down = gaussian(key_of[11], (FF, D), FF ** -0.5, 0.0625, ((0, 64),))
    return dict(hidden_in=hidden_in, mix_gain=mix_gain, w_value=w_value, w_gate=w_gate, conv_taps=conv_taps, conv_bias=conv_bias, chan_gain=chan_gain, chan_bias=chan_bias, w_back=w_back, feed_gain=feed_gain, w_up=w_up, w_down=w_down)


def rms_norm(stream, gain):
    values = stream.astype(jnp.float32)
    scaled = values * lax.rsqrt(lax.optimization_barrier(jnp.mean(values * values, axis=-1, keepdims=True)) + 1e-06)
    return (scaled * gain).astype(jnp.bfloat16)

def causal_filter(gated, conv_taps, conv_bias):
    channels = gated.shape[1]
    blocks = gated.reshape(gated.shape[0] // LEN, LEN, channels)
    padded = jnp.pad(blocks, ((0, 0), (KW - 1, 0), (0, 0)))
    result = jnp.zeros_like(blocks) + conv_bias
    for tap_index in range(KW):
        result = result + conv_taps[tap_index] * padded[:, tap_index:tap_index + LEN]
    return result.reshape(gated.shape)

def blocked_sum(left, right):
    inner = left.shape[1] // N_TP
    running = jnp.zeros((left.shape[0], right.shape[1]), jnp.float32)
    for block_index in range(N_TP):
        partial_value = jnp.dot(left[:, block_index * inner:(block_index + 1) * inner], right[block_index * inner:(block_index + 1) * inner], preferred_element_type=jnp.float32)
        running = running + partial_value.astype(jnp.bfloat16).astype(jnp.float32)
    return running

def strided_sum(left, right):
    rows = left.shape[0]
    width = right.shape[1]
    block = left.shape[1] // (N_FS * N_TP)
    left_blocks = left.reshape(rows, N_FS, N_TP, block)
    right_blocks = right.reshape(N_FS, N_TP, block, width)
    running = jnp.zeros((rows, width), jnp.float32)
    for block_index in range(N_TP):
        partial_value = jnp.dot(left_blocks[:, :, block_index].reshape(rows, N_FS * block), right_blocks[:, block_index].reshape(N_FS * block, width), preferred_element_type=jnp.float32)
        running = running + partial_value.astype(jnp.bfloat16).astype(jnp.float32)
    return running

def reference(hidden_in, mix_gain, w_value, w_gate, conv_taps, conv_bias, chan_gain, chan_bias, w_back, feed_gain, w_up, w_down):
    normed = rms_norm(hidden_in, mix_gain)
    value_proj = jnp.dot(normed, w_value, preferred_element_type=jnp.float32)
    gate_proj = jnp.dot(normed, w_gate, preferred_element_type=jnp.float32)
    gated = value_proj * jax.nn.sigmoid(gate_proj)
    filtered = causal_filter(gated, conv_taps, conv_bias)
    chan_mean = lax.optimization_barrier(jnp.mean(filtered, axis=1, keepdims=True))
    chan_var = lax.optimization_barrier(jnp.mean(filtered * filtered, axis=1, keepdims=True)) - chan_mean * chan_mean
    centred = (filtered - chan_mean) * lax.rsqrt(chan_var + 1e-05) * chan_gain + chan_bias
    mixer_act = jax.nn.silu(centred).astype(jnp.bfloat16)
    mixed = blocked_sum(mixer_act, w_back)
    second = (hidden_in.astype(jnp.float32) + mixed).astype(jnp.bfloat16)
    normed_feed = rms_norm(second, feed_gain)
    up_proj = jnp.dot(normed_feed, w_up, preferred_element_type=jnp.float32)
    hidden = jnp.square(jax.nn.relu(up_proj)).astype(jnp.bfloat16)
    feed = strided_sum(hidden, w_down)
    return (second.astype(jnp.float32) + feed).astype(jnp.bfloat16)
```

```python
import functools

import jax
import jax.numpy as jnp
from jax import lax
from jax.experimental import pallas as pl
from jax.experimental.pallas import tpu as pltpu
from jax.sharding import PartitionSpec as P

KW = 31
LEN = 128
SIDE = 4
F32 = jnp.float32
BF16 = jnp.bfloat16
UP_PIECES = 4
DOWN_PIECES = 4
PIECES = 2 + UP_PIECES + DOWN_PIECES


def kernel(
    x_hbm, mix_gain, wv_hbm, wg_hbm, taps, conv_bias, chan_gain, chan_bias, wb_hbm, feed_gain, wu_hbm, wd_hbm,
    out_hbm,
    conv_w, up_w, down_w, x_full, normed, padded, filtered, act, stat_own, stat_got,
    mix_send, mix_got, second, hidden, part_send, part_got, keep, own_sum, ret_send, ret_got, out_vmem,
    load_sem, send_sem, recv_sem, z_send, z_recv, pair_send, pair_recv, hop_send, hop_recv, out_sem,
):
    rows, half = x_hbm.shape
    features = 2 * half
    channels = wv_hbm.shape[1]
    k_rows = wv_hbm.shape[0]
    block = wu_hbm.shape[1]
    sequences = rows // LEN
    part_rows = rows // 2

    core = lax.axis_index("tp")
    other = 1 - core
    place = lax.axis_index("fs")
    z_hi = lax.axis_index("rep")
    x = lax.rem(place, SIDE)
    y = lax.rem(place // SIDE, SIDE)
    z_lo = place // (SIDE * SIDE)
    z = z_hi * 2 + z_lo
    x_next, x_prev = lax.rem(x + 1, SIDE), lax.rem(x + SIDE - 1, SIDE)
    y_next, y_prev = lax.rem(y + 1, SIDE), lax.rem(y + SIDE - 1, SIDE)
    z_next, z_prev = lax.rem(z + 1, 4), lax.rem(z + 3, 4)

    def at_x(xx):
        return {"fs": z_lo * SIDE * SIDE + y * SIDE + xx}

    def at_y(yy):
        return {"fs": z_lo * SIDE * SIDE + yy * SIDE + x}

    def at_z(zz):
        return {"rep": zz // 2, "fs": lax.rem(zz, 2) * SIDE * SIDE + y * SIDE + x}

    partner = {"tp": other}
    mesh_type = pl.DeviceIdType.MESH

    def remote(src, dst, send, recv, device):
        return pltpu.make_async_remote_copy(
            src_ref=src, dst_ref=dst, send_sem=send, recv_sem=recv, device_id=device, device_id_type=mesh_type
        )

    def of(ref, i, n):
        return pl.ds(pl.multiple_of(i * n, n), n)

    conv_row = z_lo * SIDE + y
    loads = [
        pltpu.make_async_copy(wv_hbm, conv_w.at[conv_row, of(0, x, k_rows), 0:channels], load_sem.at[0]),
        pltpu.make_async_copy(wg_hbm, conv_w.at[conv_row, of(0, x, k_rows), channels : 2 * channels], load_sem.at[1]),
        pltpu.make_async_copy(wb_hbm, conv_w.at[conv_row, of(0, x, k_rows), 2 * channels : 3 * channels], load_sem.at[2]),
        pltpu.make_async_copy(wu_hbm, up_w.at[y, :, of(0, x, block)], load_sem.at[3]),
        pltpu.make_async_copy(wd_hbm, down_w.at[y, of(0, x, block), :], load_sem.at[4]),
        pltpu.make_async_copy(x_hbm, x_full.at[:, of(0, core, half)], load_sem.at[5]),
    ]
    for load in loads:
        load.start()

    barrier = pltpu.get_barrier_semaphore()
    for device in (at_x(x_next), at_x(x_prev), at_y(y_next), at_y(y_prev), at_z(z_next), at_z(z_prev), partner):
        pl.semaphore_signal(barrier, inc=1, device_id=device, device_id_type=mesh_type)
    pl.semaphore_wait(barrier, 7)

    def span(first, size, part):
        return pl.ds(first, size) if part is None else pl.ds(first + part * (size // 2), size // 2)

    def conv_piece(first, width):
        def view(what, yy, xx, colour, part):
            cols = span(first + colour * width, width, part)
            if what == "block":
                return conv_w.at[z_lo * SIDE + yy, of(0, xx, k_rows), cols]
            if what == "row":
                return conv_w.at[z_lo * SIDE + yy, :, cols]
            return conv_w.at[pl.ds(z_lo * SIDE, SIDE), of(0, xx, k_rows), cols]

        return view

    def up_piece(index):
        size = features // UP_PIECES // 2

        def view(what, yy, xx, colour, part):
            depth = span((2 * index + colour) * size, size, part)
            if what == "block":
                return up_w.at[yy, depth, of(0, xx, block)]
            if what == "row":
                return up_w.at[yy, depth, :]
            return up_w.at[:, depth, of(0, xx, block)]

        return view

    width = half // DOWN_PIECES

    def down_piece(index):
        def view(what, yy, xx, colour, part):
            cols = span(colour * half + index * width, width, part)
            if what == "block":
                return down_w.at[yy, of(0, xx, block), cols]
            if what == "row":
                return down_w.at[yy, :, cols]
            return down_w.at[:, of(0, xx, block), cols]

        return view

    views = [conv_piece(0, channels), conv_piece(2 * channels, channels // 2)]
    views += [up_piece(i) for i in range(UP_PIECES)] + [down_piece(i) for i in range(DOWN_PIECES)]

    def step_copies(piece, step):
        view = views[piece]
        if step == 0:
            own = [("block", y, x, 0, None), ("block", y, x, 1, None)]
            pairs = [(own[0], own[0]), (own[1], own[1])]
        elif step == 1:
            pairs = [
                (("block", y, x_prev, 0, 0), ("block", y, x_next, 0, 1)),
                (("block", y_prev, x, 1, 0), ("block", y_next, x, 1, 1)),
            ]
        elif step == 2:
            pairs = [(("row", y, x, 0, None),) * 2, (("col", y, x, 1, None),) * 2]
        else:
            pairs = [
                (("row", y_prev, x, 0, 0), ("row", y_next, x, 0, 1)),
                (("col", y, x_prev, 1, 0), ("col", y, x_next, 1, 1)),
            ]
        along_x = (at_x(x_next), at_x(x_prev))
        along_y = (at_y(y_next), at_y(y_prev))
        copies = []
        for colour in range(2):
            devices = along_x if (step < 2) == (colour == 0) else along_y
            for way in range(2):
                ref = view(*pairs[colour][way])
                copies.append(
                    remote(
                        ref, ref,
                        send_sem.at[((piece * 4 + step) * 2 + colour) * 2 + way],
                        recv_sem.at[((piece * 4 + step) * 2 + colour) * 2 + way],
                        devices[way],
                    )
                )
        return copies

    flying = {}
    z_flying = {}

    def z_copies(piece, stage):
        view = views[piece]
        sets = {
            0: [(("row", y, x, 0, None), ("col", y, x, 1, None))],
            1: [
                (("row", y_prev, x, 0, None), ("col", y, x_prev, 1, None)),
                (("row", y_next, x, 0, None), ("col", y, x_next, 1, None)),
            ],
            2: [(("row", lax.rem(y + 2, SIDE), x, 0, None), ("col", y, lax.rem(x + 2, SIDE), 1, None))],
        }[stage]
        copies = []
        for number, pair in enumerate(sets):
            slot = {0: 0, 1: 1, 2: 3}[stage] + number
            for colour in range(2):
                ref = view(*pair[colour])
                index = (piece * 4 + slot) * 2 + colour
                copies.append(remote(ref, ref, z_send.at[index], z_recv.at[index], at_z((z_next, z_prev)[colour])))
        return copies

    def advance(piece):
        step = 0
        if piece in flying:
            step, copies = flying[piece]
            for copy in copies:
                copy.wait()
            step += 1
        if step < 4:
            copies = step_copies(piece, step)
            for copy in copies:
                copy.start()
            flying[piece] = (step, copies)
        if piece < 2 and step >= 2:
            copies = z_copies(piece, step - 2)
            for copy in copies:
                copy.start()
            z_flying.setdefault(piece, []).extend(copies)

    def z_wait(piece):
        for copy in z_flying[piece]:
            copy.wait()

    state = {"first": 0, "next": 2}

    def tick():
        for piece in range(state["first"], state["next"]):
            advance(piece)
        if state["next"] < PIECES:
            advance(state["next"])
            state["next"] += 1
        while state["first"] < state["next"] and flying[state["first"]][0] == 3 and state.get("done", {}).get(state["first"]):
            state["first"] += 1

    steps_done = [0] * PIECES

    def beat():
        for piece in range(PIECES):
            if 0 < steps_done[piece] <= 4:
                advance(piece)
                steps_done[piece] += 1
        for piece in range(PIECES):
            if steps_done[piece] == 0:
                advance(piece)
                steps_done[piece] = 1
                break

    x_swap = remote(x_hbm, x_full.at[:, of(0, core, half)], pair_send.at[0], pair_recv.at[0], partner)
    x_swap.start()
    loads[0].wait()
    loads[1].wait()
    beat()
    loads[2].wait()
    advance(1)
    steps_done[1] = 1
    loads[3].wait()
    loads[4].wait()
    advance(2)
    steps_done[2] = 1

    def rms(src, dst, gain, first, count, step_rows=32):
        scale = gain[...]

        def body(i, carry):
            at = pl.ds(pl.multiple_of(first + i * step_rows, step_rows), step_rows)
            values = src[at, :].astype(F32)
            mean = jnp.sum(values * values, axis=1, keepdims=True) * (1.0 / features)
            dst[at, :] = (values * lax.rsqrt(mean + 1e-6) * scale).astype(BF16)
            return carry

        lax.fori_loop(0, count // step_rows, body, 0)

    loads[5].wait()
    x_swap.wait()
    rms(x_full, normed, mix_gain, 0, rows)
    beat()
    beat()
    beat()
    padded[:, 0:32, :] = jnp.zeros((sequences, 32, channels), F32)
    beat()
    z_wait(0)

    tile = 256
    for n in range(channels // tile):
        cols = slice(n * tile, (n + 1) * tile)
        gcols = slice(channels + n * tile, channels + (n + 1) * tile)
        value = jnp.dot(normed[0:rows, :], conv_w[:, :, cols].reshape(features, tile), preferred_element_type=F32)
        gate = jnp.dot(normed[0:rows, :], conv_w[:, :, gcols].reshape(features, tile), preferred_element_type=F32)
        gated = value * jax.nn.sigmoid(gate)
        padded[:, 32 : 32 + LEN, cols] = gated.reshape(sequences, LEN, tile)
    beat()

    def filter_body(s, carry):
        at = pl.ds(pl.multiple_of(s * LEN, LEN), LEN)
        first = jnp.zeros((LEN, 128), F32)
        square = jnp.zeros((LEN, 128), F32)
        for lane in range(channels // 128):
            cols = slice(lane * 128, (lane + 1) * 128)
            slab = padded[s, :, cols]
            total = jnp.broadcast_to(conv_bias[:, cols], (LEN, 128))
            for shift in range(8):
                acc = None
                for q in range(5):
                    k = 8 * q + shift - 2
                    if 0 <= k < KW:
                        high = LEN + (8 if shift else 0)
                        term = taps[k : k + 1, cols] * slab[8 * q : 8 * q + high]
                        acc = term if acc is None else acc + term
                total = total + acc[shift : shift + LEN]
            filtered[at, cols] = total
            first = first + total
            square = square + total * total
        stat_own[0, at, :] = first
        stat_own[1, at, :] = square
        return carry

    lax.fori_loop(0, sequences, filter_body, 0)
    stat_swap = remote(stat_own, stat_got, pair_send.at[1], pair_recv.at[1], partner)
    stat_swap.start()
    beat()
    stat_swap.wait()

    def norm_body(i, carry):
        at = pl.ds(pl.multiple_of(i * 64, 64), 64)
        scale = 1.0 / (2 * channels)
        mean = jnp.sum(stat_own[0, at, :] + stat_got[0, at, :], axis=1, keepdims=True) * scale
        power = jnp.sum(stat_own[1, at, :] + stat_got[1, at, :], axis=1, keepdims=True) * scale
        spread = lax.rsqrt(power - mean * mean + 1e-5)
        centred = (filtered[at, :] - mean) * spread * chan_gain[...] + chan_bias[...]
        act[at, :] = (centred * jax.nn.sigmoid(centred)).astype(BF16)
        return carry

    lax.fori_loop(0, rows // 64, norm_body, 0)
    z_wait(1)

    def back_half(which):
        weights = conv_w[pl.ds(which * SIDE, SIDE), :, 2 * channels : 3 * channels].reshape(half, channels)
        return lax.dot_general(act[...], weights, (((1,), (1,)), ((), ())), preferred_element_type=F32)

    mix_send[...] = back_half(other).astype(BF16)
    mix_swap = remote(mix_send, mix_got, pair_send.at[2], pair_recv.at[2], partner)
    mix_swap.start()
    own_sum[...] = back_half(core)
    beat()
    mix_swap.wait()
    mine = of(0, core, half)
    mixed = own_sum[...].astype(BF16).astype(F32) + mix_got[...].astype(F32)
    second[0:rows, mine] = (x_full[:, mine].astype(F32) + mixed).astype(BF16)

    own_rows = second.at[0:rows, mine]
    second_swap = remote(own_rows, own_rows, pair_send.at[3], pair_recv.at[3], partner)
    low, high = pl.ds(0, part_rows), pl.ds(part_rows, part_rows)
    from_prev, from_next = pl.ds(rows, part_rows), pl.ds(rows + part_rows, part_rows)
    hops = [
        remote(second.at[low, mine], second.at[from_prev, mine], hop_send.at[0], hop_recv.at[0], at_z(z_next)),
        remote(second.at[high, mine], second.at[from_next, mine], hop_send.at[1], hop_recv.at[1], at_z(z_prev)),
    ]
    for hop in hops:
        hop.start()
    second_swap.start()
    beat()
    second_swap.wait()

    def up(first):
        at = pl.ds(first, rows)

        def body(i, carry):
            product = jnp.dot(normed[at, :], up_w[i], preferred_element_type=F32)
            positive = jnp.maximum(product, 0.0)
            hidden[at, pl.ds(pl.multiple_of(i * SIDE * block, SIDE * block), SIDE * block)] = (positive * positive).astype(BF16)
            return carry

        lax.fori_loop(0, SIDE, body, 0)

    rms(second, normed, feed_gain, 0, rows)
    up(0)
    for hop in hops:
        hop.wait()
    foreign = second.at[pl.ds(rows, rows), mine]
    foreign_swap = remote(foreign, foreign, pair_send.at[4], pair_recv.at[4], partner)
    foreign_swap.start()
    beat()
    foreign_swap.wait()
    rms(second, normed, feed_gain, rows, rows)
    up(rows)
    beat()

    def down(index):
        def product(which, first):
            cols = pl.ds(pl.multiple_of(which * half + index * width, width), width)
            weights = down_w[:, :, cols].reshape(SIDE * SIDE * block, width)
            return jnp.dot(hidden[pl.ds(first, rows), :], weights, preferred_element_type=F32)

        cols = pl.ds(index * width, width)
        for first in (0, rows):
            part_send[pl.ds(first, rows), cols] = product(other, first).astype(BF16)
        swap = remote(part_send.at[:, cols], part_got.at[:, cols], pair_send.at[5 + index], pair_recv.at[5 + index], partner)
        swap.start()
        for first in (rows, 0):
            keep[pl.ds(first, rows), :] = product(core, first)
        swap.wait()
        ret_send[:, cols] = (keep[pl.ds(rows, rows), :] + part_got[pl.ds(rows, rows), cols].astype(F32)).astype(BF16)
        back = [
            remote(ret_send.at[low, cols], ret_got.at[low, cols], hop_send.at[2 + 2 * index], hop_recv.at[2 + 2 * index], at_z(z_prev)),
            remote(ret_send.at[high, cols], ret_got.at[high, cols], hop_send.at[3 + 2 * index], hop_recv.at[3 + 2 * index], at_z(z_next)),
        ]
        for copy in back:
            copy.start()
        own_sum[:, cols] = keep[pl.ds(0, rows), :] + part_got[pl.ds(0, rows), cols].astype(F32)
        return back

    outs = []

    def finish(index, back):
        for copy in back:
            copy.wait()
        cols = pl.ds(index * width, width)
        there = pl.ds(pl.multiple_of(core * half + index * width, width), width)
        total = second[0:rows, there].astype(F32) + own_sum[:, cols] + ret_got[:, cols].astype(F32)
        out_vmem[:, cols] = total.astype(BF16)
        copy = pltpu.make_async_copy(out_vmem.at[:, cols], out_hbm.at[:, cols], out_sem.at[index])
        copy.start()
        outs.append(copy)

    waiting = None
    for index in range(DOWN_PIECES):
        while steps_done[2 + UP_PIECES + index] < 5:
            beat()
        back = down(index)
        if waiting is not None:
            finish(index - 1, waiting)
        waiting = back
    finish(DOWN_PIECES - 1, waiting)
    for copy in outs:
        copy.wait()


def shards(
    hidden_in, mix_gain, w_value, w_gate, conv_taps, conv_bias, chan_gain, chan_bias, w_back, feed_gain, w_up, w_down
):
    rows, half = hidden_in.shape
    features = 2 * half
    channels = w_value.shape[1]
    block = w_up.shape[1]
    plane = SIDE * SIDE
    sequences = rows // LEN
    vmem = pl.BlockSpec(memory_space=pltpu.VMEM)
    hbm = pl.BlockSpec(memory_space=pl.ANY)
    dma = pltpu.SemaphoreType.DMA
    width = half // DOWN_PIECES
    scratch = [
        pltpu.VMEM((2 * SIDE, SIDE * w_value.shape[0], 3 * channels), BF16),
        pltpu.VMEM((SIDE, features, SIDE * block), BF16),
        pltpu.VMEM((SIDE, SIDE * block, features), BF16),
        pltpu.VMEM((rows, features), BF16),
        pltpu.VMEM((2 * rows, features), BF16),
        pltpu.VMEM((sequences, 32 + LEN, channels), F32),
        pltpu.VMEM((rows, channels), F32),
        pltpu.VMEM((rows, channels), BF16),
        pltpu.VMEM((2, rows, 128), F32),
        pltpu.VMEM((2, rows, 128), F32),
        pltpu.VMEM((rows, half), BF16),
        pltpu.VMEM((rows, half), BF16),
        pltpu.VMEM((2 * rows, features), BF16),
        pltpu.VMEM((2 * rows, plane * block), BF16),
        pltpu.VMEM((2 * rows, half), BF16),
        pltpu.VMEM((2 * rows, half), BF16),
        pltpu.VMEM((2 * rows, width), F32),
        pltpu.VMEM((rows, half), F32),
        pltpu.VMEM((rows, half), BF16),
        pltpu.VMEM((rows, half), BF16),
        pltpu.VMEM((rows, half), BF16),
        dma((6,)),
        dma((PIECES * 16,)),
        dma((PIECES * 16,)),
        dma((16,)),
        dma((16,)),
        dma((5 + DOWN_PIECES,)),
        dma((5 + DOWN_PIECES,)),
        dma((2 + 2 * DOWN_PIECES,)),
        dma((2 + 2 * DOWN_PIECES,)),
        dma((DOWN_PIECES,)),
    ]
    return pl.pallas_call(
        kernel,
        out_shape=jax.ShapeDtypeStruct((rows, half), BF16),
        in_specs=[hbm, vmem, hbm, hbm, vmem, vmem, vmem, vmem, hbm, vmem, hbm, hbm],
        out_specs=hbm,
        scratch_shapes=scratch,
        compiler_params=pltpu.CompilerParams(
            collective_id=0, has_side_effects=True, vmem_limit_bytes=67043328
        ),
    )(
        hidden_in,
        mix_gain[None, :],
        w_value,
        w_gate,
        conv_taps,
        conv_bias[None, :],
        chan_gain[None, :],
        chan_bias[None, :],
        w_back.T,
        feed_gain[None, :],
        w_up,
        w_down,
    )


def solution(mesh):
    placed = (
        P(("rep", "fs"), "tp"),
        P(),
        P("fs", "tp"),
        P("fs", "tp"),
        P(None, "tp"),
        P("tp"),
        P("tp"),
        P("tp"),
        P("tp", "fs"),
        P(),
        P(None, ("fs", "tp")),
        P(("fs", "tp"), None),
    )
    return jax.shard_map(
        shards, mesh=mesh, in_specs=placed, out_specs=P(("rep", "fs"), "tp"), check_vma=False
    )
```

```python
import functools

import jax
import jax.numpy as jnp
from jax import lax
from jax.experimental import pallas as pl
from jax.experimental.pallas import tpu as pltpu
from jax.sharding import PartitionSpec as P

KW = 31
LEN = 128
SIDE = 4
F32 = jnp.float32
BF16 = jnp.bfloat16
UP_PIECES = 4
DOWN_WIDTHS = (256, 256, 128, 128, 128, 128)
DOWN_FIRST = (0, 256, 512, 640, 768, 896)
DOWN_PIECES = len(DOWN_WIDTHS)
PIECES = 2 + UP_PIECES + DOWN_PIECES
UNITS = (1, 0.5) + (4 / UP_PIECES,) * UP_PIECES + tuple(width / 256 for width in DOWN_WIDTHS)

ORDER = (
    "a1", "a0", "a3", "a2", "a7", "a0", "a1", "a10", "a5", "rmsx", "a4", "a6", "a0", "a9", "a3", "a1", "z00", "a4",
    "a0", "z10", "a5", "a2", "a8", "a6", "a3", "a1", "a11", "z01", "a5", "a2", "a4", "a7", "a0", "z02", "vg0", "a1",
    "z11", "a9", "a11", "a3", "zw0", "a5", "z12", "vg1", "filter", "a2", "statw", "chan", "a4", "zw1", "a8", "bo",
    "bw", "a7", "mixw", "second", "a2", "a10", "secw", "a5", "a6", "a4", "rms", "a3", "a8", "upa", "upb", "a7",
    "hopw", "a6", "forw", "rmsf", "a9", "a8", "a10", "upfa", "a7", "upfb", "a6", "a11", "down0", "a9", "down1", "a8",
    "a10", "down2", "a11", "a9", "down3", "a10", "down4", "a11", "down5",
)


def kernel(
    x_hbm, mix_gain, wv_hbm, wg_hbm, taps, conv_bias, chan_gain, chan_bias, wb_hbm, feed_gain, wu_hbm, wd_hbm,
    out_hbm,
    conv_w, up_w, down_w, x_full, normed, padded, filtered, act, stat_own, stat_got,
    second, hidden, part, part_got, own_sum, ret_send, ret_got, out_vmem,
    load_sem, send_sem, recv_sem, z_send, z_recv, pair_send, pair_recv, hop_send, hop_recv, out_sem,
):
    rows, half = x_hbm.shape
    features = 2 * half
    channels = wv_hbm.shape[1]
    k_rows = wv_hbm.shape[0]
    block = wu_hbm.shape[1]
    sequences = rows // LEN
    part_rows = rows // 2

    core = lax.axis_index("tp")
    other = 1 - core
    place = lax.axis_index("fs")
    z_hi = lax.axis_index("rep")
    x = lax.rem(place, SIDE)
    y = lax.rem(place // SIDE, SIDE)
    z_lo = place // (SIDE * SIDE)
    z = z_hi * 2 + z_lo
    x_next, x_prev = lax.rem(x + 1, SIDE), lax.rem(x + SIDE - 1, SIDE)
    y_next, y_prev = lax.rem(y + 1, SIDE), lax.rem(y + SIDE - 1, SIDE)
    z_next, z_prev = lax.rem(z + 1, 4), lax.rem(z + 3, 4)

    def at_x(xx):
        return {"fs": z_lo * SIDE * SIDE + y * SIDE + xx}

    def at_y(yy):
        return {"fs": z_lo * SIDE * SIDE + yy * SIDE + x}

    def at_z(zz):
        return {"rep": zz // 2, "fs": lax.rem(zz, 2) * SIDE * SIDE + y * SIDE + x}

    partner = {"tp": other}
    mesh_type = pl.DeviceIdType.MESH

    def remote(src, dst, send, recv, device):
        return pltpu.make_async_remote_copy(
            src_ref=src, dst_ref=dst, send_sem=send, recv_sem=recv, device_id=device, device_id_type=mesh_type
        )

    def of(ref, i, n):
        return pl.ds(pl.multiple_of(i * n, n), n)

    conv_row = z_lo * SIDE + y
    loads = [
        pltpu.make_async_copy(wv_hbm, conv_w.at[conv_row, of(0, x, k_rows), 0:channels], load_sem.at[0]),
        pltpu.make_async_copy(wg_hbm, conv_w.at[conv_row, of(0, x, k_rows), channels : 2 * channels], load_sem.at[1]),
        pltpu.make_async_copy(wb_hbm, conv_w.at[conv_row, of(0, x, k_rows), 2 * channels : 3 * channels], load_sem.at[2]),
        pltpu.make_async_copy(wu_hbm, up_w.at[y, :, of(0, x, block)], load_sem.at[3]),
        pltpu.make_async_copy(x_hbm, x_full.at[:, of(0, core, half)], load_sem.at[4]),
    ]
    for index in range(DOWN_PIECES):
        width, first = DOWN_WIDTHS[index], DOWN_FIRST[index]
        for h in range(2):
            src = wd_hbm.at[:, pl.ds(h * half + first, width)]
            dst = down_w.at[y, of(0, x, block), pl.ds(2 * first + h * width, width)]
            loads.append(pltpu.make_async_copy(src, dst, load_sem.at[5]))
    for load in loads:
        load.start()

    barrier = pltpu.get_barrier_semaphore()
    for device in (at_x(x_next), at_x(x_prev), at_y(y_next), at_y(y_prev), at_z(z_next), at_z(z_prev), partner):
        pl.semaphore_signal(barrier, inc=1, device_id=device, device_id_type=mesh_type)
    with jax.named_scope("barrier"):
        pl.semaphore_wait(barrier, 7)

    def span(first, size, part):
        return pl.ds(first, size) if part is None else pl.ds(first + part * (size // 2), size // 2)

    def conv_piece(first, width):
        def view(what, yy, xx, colour, part):
            cols = span(first + colour * width, width, part)
            if what == "block":
                return conv_w.at[z_lo * SIDE + yy, of(0, xx, k_rows), cols]
            if what == "row":
                return conv_w.at[z_lo * SIDE + yy, :, cols]
            return conv_w.at[pl.ds(z_lo * SIDE, SIDE), of(0, xx, k_rows), cols]

        return view

    def up_piece(index):
        size = features // UP_PIECES // 2

        def view(what, yy, xx, colour, part):
            depth = span((2 * index + colour) * size, size, part)
            if what == "block":
                return up_w.at[yy, depth, of(0, xx, block)]
            if what == "row":
                return up_w.at[yy, depth, :]
            return up_w.at[:, depth, of(0, xx, block)]

        return view

    def down_piece(index):
        width, first = DOWN_WIDTHS[index], DOWN_FIRST[index]

        def view(what, yy, xx, colour, part):
            cols = pl.ds(2 * first + colour * width, width)
            size = block if part is None else block // 2
            rows_of_block = pl.ds(pl.multiple_of(xx * block + (part or 0) * size, size), size)
            if what == "block":
                return down_w.at[yy, rows_of_block, cols]
            if what == "row":
                return down_w.at[yy, span(0, SIDE * block, part), cols]
            return down_w.at[:, rows_of_block, cols]

        return view

    views = [conv_piece(0, channels), conv_piece(2 * channels, channels // 2)]
    views += [up_piece(i) for i in range(UP_PIECES)] + [down_piece(i) for i in range(DOWN_PIECES)]

    def step_copies(piece, step):
        view = views[piece]
        if step == 0:
            own = [("block", y, x, 0, None), ("block", y, x, 1, None)]
            pairs = [(own[0], own[0]), (own[1], own[1])]
        elif step == 1:
            pairs = [
                (("block", y, x_prev, 0, 0), ("block", y, x_next, 0, 1)),
                (("block", y_prev, x, 1, 0), ("block", y_next, x, 1, 1)),
            ]
        elif step == 2:
            pairs = [(("row", y, x, 0, None),) * 2, (("col", y, x, 1, None),) * 2]
        else:
            pairs = [
                (("row", y_prev, x, 0, 0), ("row", y_next, x, 0, 1)),
                (("col", y, x_prev, 1, 0), ("col", y, x_next, 1, 1)),
            ]
        along_x = (at_x(x_next), at_x(x_prev))
        along_y = (at_y(y_next), at_y(y_prev))
        copies = []
        for colour in range(2):
            devices = along_x if (step < 2) == (colour == 0) else along_y
            for way in range(2):
                ref = view(*pairs[colour][way])
                copies.append(remote(ref, ref, send_sem.at[piece], recv_sem.at[piece * 4 + step], devices[way]))
        return copies

    flying = {}

    def z_copies(piece, stage):
        view = views[piece]
        sets = {
            0: [(("row", y, x, 0, None), ("col", y, x, 1, None))],
            1: [
                (("row", y_prev, x, 0, None), ("col", y, x_prev, 1, None)),
                (("row", y_next, x, 0, None), ("col", y, x_next, 1, None)),
            ],
            2: [(("row", lax.rem(y + 2, SIDE), x, 0, None), ("col", y, lax.rem(x + 2, SIDE), 1, None))],
        }[stage]
        copies = []
        for pair in sets:
            for colour in range(2):
                ref = view(*pair[colour])
                copies.append(remote(ref, ref, z_send.at[piece], z_recv.at[piece], at_z((z_next, z_prev)[colour])))
        return copies

    counts = {}

    def advance(piece):
        counts[piece] = counts.get(piece, 0) + 1
        step = 0
        if piece in flying:
            step = flying[piece]
            with jax.named_scope(f"wait_{piece}_{step}"):
                kib = int(4 * UNITS[piece] * 64 * (1, 0.5, 4, 2)[step])
                four = up_w.at[0, 0:kib, :]
                pltpu.make_async_copy(four, four, recv_sem.at[piece * 4 + step]).wait()
                pltpu.make_async_copy(four, four, send_sem.at[piece]).wait()
            step += 1
        if step < 4:
            copies = step_copies(piece, step)
            for copy in copies:
                copy.start()
            flying[piece] = step

    def z_go(piece, stage):
        for copy in z_copies(piece, stage):
            copy.start()

    def z_wait(piece):
        first = 2 * channels * piece
        whole = conv_w.at[pl.ds((1 - z_lo) * SIDE, SIDE), :, pl.ds(first, (2 - piece) * channels)]
        pltpu.make_async_copy(whole, whole, z_recv.at[piece]).wait()
        pltpu.make_async_copy(whole, whole, z_send.at[piece]).wait()

    ups = list(range(2, 2 + UP_PIECES))
    downs = list(range(2 + UP_PIECES, PIECES))

    def rms(src, dst, gain, first, count, step_rows=32):
        scale = gain[...]

        def body(i, carry):
            at = pl.ds(pl.multiple_of(first + i * step_rows, step_rows), step_rows)
            values = src[at, :].astype(F32)
            mean = jnp.sum(values * values, axis=1, keepdims=True) * (1.0 / features)
            dst[at, :] = (values * lax.rsqrt(mean + 1e-6) * scale).astype(BF16)
            return carry

        lax.fori_loop(0, count // step_rows, body, 0)

    mine = of(0, core, half)
    own, foreign = pl.ds(0, rows), pl.ds(rows, rows)
    low, high = pl.ds(0, part_rows), pl.ds(part_rows, part_rows)
    from_prev, from_next = pl.ds(rows, part_rows), pl.ds(rows + part_rows, part_rows)
    mix_send, mix_got = part.at[0, 0:rows, :], part_got.at[0:rows, :]
    x_swap = remote(x_hbm, x_full.at[:, mine], pair_send.at[0], pair_recv.at[0], partner)
    stat_swap = remote(stat_own, stat_got, pair_send.at[1], pair_recv.at[1], partner)
    mix_swap = remote(mix_send, mix_got, pair_send.at[2], pair_recv.at[2], partner)
    second_swap = remote(second.at[own, mine], second.at[own, mine], pair_send.at[3], pair_recv.at[3], partner)
    foreign_swap = remote(second.at[foreign, mine], second.at[foreign, mine], pair_send.at[4], pair_recv.at[4], partner)
    hops = [
        remote(second.at[low, mine], second.at[from_prev, mine], hop_send.at[0], hop_recv.at[0], at_z(z_next)),
        remote(second.at[high, mine], second.at[from_next, mine], hop_send.at[0], hop_recv.at[0], at_z(z_prev)),
    ]

    def first_norm():
        loads[4].wait()
        x_swap.wait()
        rms(x_full, normed, mix_gain, 0, rows)
        padded[:, 0:32, :] = jnp.zeros((sequences, 32, channels), F32)

    tile = 256

    def plane_dot(which, cols):
        at = pl.ds(pl.multiple_of(which * half, half), half)
        weights = conv_w[pl.ds(which * SIDE, SIDE), :, cols].reshape(half, tile)
        return jnp.dot(normed[0:rows, at], weights, preferred_element_type=F32)

    def value_gate_own():
        for n in range(2 * channels // tile):
            cols = slice(n * tile, (n + 1) * tile)
            own_sum[:, cols] = plane_dot(z_lo, cols)

    def value_gate_rest():
        for n in range(channels // tile):
            cols = slice(n * tile, (n + 1) * tile)
            gcols = slice(channels + n * tile, channels + (n + 1) * tile)
            value = own_sum[:, cols] + plane_dot(1 - z_lo, cols)
            gate = own_sum[:, gcols] + plane_dot(1 - z_lo, gcols)
            gated = value * jax.nn.sigmoid(gate)
            padded[:, 32 : 32 + LEN, cols] = gated.reshape(sequences, LEN, tile)

    def causal_filter():
        def body(s, carry):
            at = pl.ds(pl.multiple_of(s * LEN, LEN), LEN)
            first = jnp.zeros((LEN, 128), F32)
            square = jnp.zeros((LEN, 128), F32)
            for lane in range(channels // 128):
                cols = slice(lane * 128, (lane + 1) * 128)
                slab = padded[s, :, cols]
                total = jnp.broadcast_to(conv_bias[:, cols], (LEN, 128))
                for shift in range(8):
                    acc = None
                    for q in range(5):
                        k = 8 * q + shift - 2
                        if 0 <= k < KW:
                            tall = LEN + (8 if shift else 0)
                            term = taps[k : k + 1, cols] * slab[8 * q : 8 * q + tall]
                            acc = term if acc is None else acc + term
                    total = total + acc[shift : shift + LEN]
                filtered[at, cols] = total
                first = first + total
                square = square + total * total
            stat_own[0, at, :] = first
            stat_own[1, at, :] = square
            return carry

        lax.fori_loop(0, sequences, body, 0)
        stat_swap.start()

    def channel_norm():
        def body(i, carry):
            at = pl.ds(pl.multiple_of(i * 64, 64), 64)
            scale = 1.0 / (2 * channels)
            mean = jnp.sum(stat_own[0, at, :] + stat_got[0, at, :], axis=1, keepdims=True) * scale
            power = jnp.sum(stat_own[1, at, :] + stat_got[1, at, :], axis=1, keepdims=True) * scale
            spread = lax.rsqrt(power - mean * mean + 1e-5)
            centred = (filtered[at, :] - mean) * spread * chan_gain[...] + chan_bias[...]
            act[at, :] = (centred * jax.nn.sigmoid(centred)).astype(BF16)
            return carry

        lax.fori_loop(0, rows // 64, body, 0)

    def back_half(which):
        weights = conv_w[pl.ds(which * SIDE, SIDE), :, 2 * channels : 3 * channels].reshape(half, channels)
        return lax.dot_general(act[...], weights, (((1,), (1,)), ((), ())), preferred_element_type=F32)

    def back_other():
        mix_send[...] = back_half(other).astype(BF16)
        mix_swap.start()

    def back_own():
        own_sum[...] = back_half(core)

    def residual():
        mixed = own_sum[...].astype(BF16).astype(F32) + mix_got[...].astype(F32)
        second[own, mine] = (x_full[:, mine].astype(F32) + mixed).astype(BF16)
        for hop in hops:
            hop.start()
        second_swap.start()

    def up(first, begin, end):
        at = pl.ds(first, rows)

        def body(i, carry):
            product = jnp.dot(normed[at, :], up_w[i], preferred_element_type=F32)
            positive = jnp.maximum(product, 0.0)
            hidden[at, pl.ds(pl.multiple_of(i * SIDE * block, SIDE * block), SIDE * block)] = (positive * positive).astype(BF16)
            return carry

        lax.fori_loop(begin, end, body, 0)

    def arrived():
        both = second.at[foreign, mine]
        pltpu.make_async_copy(both, both, hop_recv.at[0]).wait()
        pltpu.make_async_copy(both, both, hop_send.at[0]).wait()
        foreign_swap.start()

    swaps = {}

    def down(index):
        width, first = DOWN_WIDTHS[index], DOWN_FIRST[index]
        cols = pl.ds(first, width)
        depth = SIDE * SIDE * block
        swaps[index] = []
        for number, at in enumerate((foreign, own)):

            def body(i, carry):
                chunk = pl.ds(pl.multiple_of(at.start + i * part_rows, part_rows), part_rows)
                weights = down_w[:, :, pl.ds(2 * first, 2 * width)].reshape(depth, 2 * width)
                product = jnp.dot(hidden[chunk, :], weights, preferred_element_type=F32).astype(BF16)
                part[0, chunk, cols] = product[:, :width]
                part[1, chunk, cols] = product[:, width:]
                return carry

            lax.fori_loop(0, 2, body, 0)
            slot = 5 + 2 * index + number
            swap = remote(part.at[other, at, cols], part_got.at[at, cols], pair_send.at[5 if number == 0 else 6 + index % 2], pair_recv.at[slot], partner)
            swap.start()
            swaps[index].append(swap)

    def send_back(index):
        width, first = DOWN_WIDTHS[index], DOWN_FIRST[index]
        cols = pl.ds(first, width)
        swaps[index][0].wait()
        ret_send[:, cols] = (part[core, foreign, cols].astype(F32) + part_got[foreign, cols].astype(F32)).astype(BF16)
        for at, device in ((low, at_z(z_prev)), (high, at_z(z_next))):
            slot = 1 + index
            back = remote(ret_send.at[at, cols], ret_got.at[at, cols], hop_send.at[slot], hop_recv.at[slot], device)
            back.start()

    def sum_own(index):
        width, first = DOWN_WIDTHS[index], DOWN_FIRST[index]
        cols = pl.ds(first, width)
        swaps[index][1].wait()
        there = pl.ds(pl.multiple_of(core * half + first, 128), width)
        own_sum[:, cols] = (
            second[own, there].astype(F32) + part[core, own, cols].astype(F32) + part_got[own, cols].astype(F32)
        )

    def finish(index):
        width, first = DOWN_WIDTHS[index], DOWN_FIRST[index]
        cols = pl.ds(first, width)
        both = ret_got.at[:, cols]
        pltpu.make_async_copy(both, both, hop_recv.at[1 + index]).wait()
        pltpu.make_async_copy(both, both, hop_send.at[1 + index]).wait()
        out_vmem[:, cols] = (own_sum[:, cols] + ret_got[:, cols].astype(F32)).astype(BF16)
        copy = pltpu.make_async_copy(out_vmem.at[:, cols], out_hbm.at[:, cols], out_sem.at[0])
        copy.start()

    def down_step(index):
        down(index)
        send_back(index)
        if index:
            sum_own(index - 1)
        if index > 1:
            finish(index - 2)

    actions = dict(
        rmsx=first_norm,
        vg0=value_gate_own,
        zw0=lambda: z_wait(0),
        vg1=value_gate_rest,
        filter=causal_filter,
        statw=stat_swap.wait,
        chan=channel_norm,
        zw1=lambda: z_wait(1),
        bo=back_other,
        bw=back_own,
        mixw=mix_swap.wait,
        second=residual,
        secw=second_swap.wait,
        rms=lambda: rms(second, normed, feed_gain, 0, rows),
        upa=lambda: up(0, 0, SIDE // 2),
        upb=lambda: up(0, SIDE // 2, SIDE),
        hopw=arrived,
        forw=foreign_swap.wait,
        rmsf=lambda: rms(second, normed, feed_gain, rows, rows),
        upfa=lambda: up(rows, 0, SIDE // 2),
        upfb=lambda: up(rows, SIDE // 2, SIDE),
    )
    for index in range(DOWN_PIECES):
        actions[f"down{index}"] = functools.partial(down_step, index)

    first_load = {0: (0, 1), 1: (2,)}
    first_load.update({piece: (3,) for piece in ups})
    first_load.update({piece: (5,) for piece in downs})
    whole_down = down_w.at[y, of(0, x, block), :]
    loads[5:] = [pltpu.make_async_copy(whole_down, whole_down, load_sem.at[5])]
    loaded = set()

    x_swap.start()
    for name in ORDER:
        if name[0] == "a" and name[1:].isdigit():
            piece = int(name[1:])
            for number in first_load[piece]:
                if number not in loaded:
                    loads[number].wait()
                    loaded.add(number)
            advance(piece)
        elif name[0] == "z" and name[1:].isdigit():
            z_go(int(name[1]), int(name[2]))
        else:
            with jax.named_scope(name):
                actions[name]()

    sum_own(DOWN_PIECES - 1)
    finish(DOWN_PIECES - 2)
    with jax.named_scope("last"):
        finish(DOWN_PIECES - 1)
        pltpu.make_async_copy(out_vmem, out_hbm, out_sem.at[0]).wait()
    assert all(counts[piece] == 5 for piece in range(PIECES)), counts


def shards(
    hidden_in, mix_gain, w_value, w_gate, conv_taps, conv_bias, chan_gain, chan_bias, w_back, feed_gain, w_up, w_down
):
    rows, half = hidden_in.shape
    features = 2 * half
    channels = w_value.shape[1]
    block = w_up.shape[1]
    plane = SIDE * SIDE
    sequences = rows // LEN
    vmem = pl.BlockSpec(memory_space=pltpu.VMEM)
    hbm = pl.BlockSpec(memory_space=pl.ANY)
    dma = pltpu.SemaphoreType.DMA
    scratch = [
        pltpu.VMEM((2 * SIDE, SIDE * w_value.shape[0], 3 * channels), BF16),
        pltpu.VMEM((SIDE, features, SIDE * block), BF16),
        pltpu.VMEM((SIDE, SIDE * block, features), BF16),
        pltpu.VMEM((rows, features), BF16),
        pltpu.VMEM((2 * rows, features), BF16),
        pltpu.VMEM((sequences, 32 + LEN, channels), F32),
        pltpu.VMEM((rows, channels), F32),
        pltpu.VMEM((rows, channels), BF16),
        pltpu.VMEM((2, rows, 128), F32),
        pltpu.VMEM((2, rows, 128), F32),
        pltpu.VMEM((2 * rows, features), BF16),
        pltpu.VMEM((2 * rows, plane * block), BF16),
        pltpu.VMEM((2, 2 * rows, half), BF16),
        pltpu.VMEM((2 * rows, half), BF16),
        pltpu.VMEM((rows, half), F32),
        pltpu.VMEM((rows, half), BF16),
        pltpu.VMEM((rows, half), BF16),
        pltpu.VMEM((rows, half), BF16),
        dma((6,)),
        dma((PIECES,)),
        dma((PIECES * 4,)),
        dma((2,)),
        dma((2,)),
        dma((8,)),
        dma((5 + 2 * DOWN_PIECES,)),
        dma((1 + DOWN_PIECES,)),
        dma((1 + DOWN_PIECES,)),
        dma((1,)),
    ]
    return pl.pallas_call(
        kernel,
        out_shape=jax.ShapeDtypeStruct((rows, half), BF16),
        in_specs=[hbm, vmem, hbm, hbm, vmem, vmem, vmem, vmem, hbm, vmem, hbm, hbm],
        out_specs=hbm,
        scratch_shapes=scratch,
        compiler_params=pltpu.CompilerParams(
            collective_id=0, has_side_effects=True, vmem_limit_bytes=67043328
        ),
    )(
        hidden_in,
        mix_gain[None, :],
        w_value,
        w_gate,
        conv_taps,
        conv_bias[None, :],
        chan_gain[None, :],
        chan_bias[None, :],
        w_back.T,
        feed_gain[None, :],
        w_up,
        w_down,
    )


def solution(mesh):
    placed = (
        P(("rep", "fs"), "tp"),
        P(),
        P("fs", "tp"),
        P("fs", "tp"),
        P(None, "tp"),
        P("tp"),
        P("tp"),
        P("tp"),
        P("tp", "fs"),
        P(),
        P(None, ("fs", "tp")),
        P(("fs", "tp"), None),
    )
    return jax.shard_map(
        shards, mesh=mesh, in_specs=placed, out_specs=P(("rep", "fs"), "tp"), check_vma=False
    )
```

```python
import functools

import jax
import jax.numpy as jnp
from jax import lax
from jax.experimental import pallas as pl
from jax.experimental.pallas import tpu as pltpu
from jax.sharding import PartitionSpec as P

KW = 31
LEN = 128
SIDE = 4
F32 = jnp.float32
BF16 = jnp.bfloat16
UP_PIECES = 4
SPLIT = 0
DOWN_WIDTHS = (256, 256, 256, 128, 128)
DOWN_FIRST = (0, 256, 512, 768, 896)
DOWN_PIECES = len(DOWN_WIDTHS)
PIECES = 2 + UP_PIECES + DOWN_PIECES
UNITS = (1, 0.5) + (4 / UP_PIECES,) * UP_PIECES
UNITS += tuple(width / 256 / (2 if i == SPLIT else 1) for i, width in enumerate(DOWN_WIDTHS))

ORDER = (
    "a1", "a0", "a6", "a5", "a2", "rmsx", "a9", "a0", "a1", "a6", "a3", "a8", "a4", "a0", "a2", "a1", "a6", "z00",
    "a9", "a5", "z10", "a0", "z01", "a1", "a3", "a7", "a6", "a5", "a3", "a0", "a1", "a4", "z02", "z11", "vg0", "a2",
    "a7", "a6", "zw0", "vg1", "z12", "a4", "a3", "y0", "filter", "statw", "y1", "a5", "chan", "zw1", "bo", "bw",
    "a2", "mixw", "second", "a4", "a8", "a5", "secw", "a10", "a7", "y2", "a3", "rms", "a2", "a4", "upa", "a10", "y3",
    "a9", "upb", "hopw", "a8", "forw", "a10", "a7", "rmsf", "upfa", "upfb", "a8", "down0", "a9", "a10", "a7",
    "down1", "a8", "down2", "a10", "a9", "down3", "down4",
)


def kernel(
    x_hbm, mix_gain_hbm, wv_hbm, wg_hbm, taps_hbm, conv_bias_hbm, chan_gain_hbm, chan_bias_hbm, wb_hbm,
    feed_gain_hbm, wu_hbm, wd_hbm,
    out_vmem,
    conv_w, up_w, down_w, x_full, normed, padded, filtered, act, stat_own, stat_got,
    mix_gain, taps, conv_bias, chan_gain, chan_bias, feed_gain,
    second, hidden, part, part_got, own_sum, ret_send, ret_got,
    relay, load_sem, send_sem, recv_sem, z_send, z_recv, pair_send, pair_recv, hop_send, hop_recv, y_send, y_recv,
):
    rows, half = x_hbm.shape
    features = 2 * half
    channels = wv_hbm.shape[1]
    k_rows = wv_hbm.shape[0]
    block = wu_hbm.shape[1]
    sequences = rows // LEN
    part_rows = rows // 2

    core = lax.axis_index("tp")
    other = 1 - core
    place = lax.axis_index("fs")
    z_hi = lax.axis_index("rep")
    x = lax.rem(place, SIDE)
    y = lax.rem(place // SIDE, SIDE)
    z_lo = place // (SIDE * SIDE)
    z = z_hi * 2 + z_lo
    x_next, x_prev = lax.rem(x + 1, SIDE), lax.rem(x + SIDE - 1, SIDE)
    y_next, y_prev = lax.rem(y + 1, SIDE), lax.rem(y + SIDE - 1, SIDE)
    z_next, z_prev = lax.rem(z + 1, 4), lax.rem(z + 3, 4)

    def at_x(xx):
        return {"fs": z_lo * SIDE * SIDE + y * SIDE + xx}

    def at_y(yy):
        return {"fs": z_lo * SIDE * SIDE + yy * SIDE + x}

    def at_z(zz):
        return {"rep": zz // 2, "fs": lax.rem(zz, 2) * SIDE * SIDE + y * SIDE + x}

    partner = {"tp": other}
    mesh_type = pl.DeviceIdType.MESH

    def remote(src, dst, send, recv, device):
        return pltpu.make_async_remote_copy(
            src_ref=src, dst_ref=dst, send_sem=send, recv_sem=recv, device_id=device, device_id_type=mesh_type
        )

    def of(ref, i, n):
        return pl.ds(pl.multiple_of(i * n, n), n)

    conv_row = z_lo * SIDE + y
    loads = [
        pltpu.make_async_copy(wv_hbm, conv_w.at[conv_row, of(0, x, k_rows), 0:channels], load_sem.at[0]),
        pltpu.make_async_copy(wg_hbm, conv_w.at[conv_row, of(0, x, k_rows), channels : 2 * channels], load_sem.at[1]),
        pltpu.make_async_copy(wb_hbm, conv_w.at[conv_row, of(0, x, k_rows), 2 * channels : 3 * channels], load_sem.at[2]),
        pltpu.make_async_copy(wu_hbm, up_w.at[y, :, of(0, x, block)], load_sem.at[3]),
        pltpu.make_async_copy(x_hbm, x_full.at[:, of(0, core, half)], load_sem.at[4]),
    ]
    for index in range(DOWN_PIECES):
        width, first = DOWN_WIDTHS[index], DOWN_FIRST[index]
        for h in range(2):
            size, shift, sem = width, 0, 5
            if index == SPLIT:
                size, sem = width // 2, 12
                shift = z_hi * size
            src = wd_hbm.at[:, pl.ds(pl.multiple_of(h * half + first + shift, 128), size)]
            dst = down_w.at[y, of(0, x, block), pl.ds(pl.multiple_of(2 * first + h * width + shift, 128), size)]
            loads.append(pltpu.make_async_copy(src, dst, load_sem.at[sem]))
    small = [(mix_gain_hbm, mix_gain), (taps_hbm, taps), (conv_bias_hbm, conv_bias)]
    small += [(chan_gain_hbm, chan_gain), (chan_bias_hbm, chan_bias), (feed_gain_hbm, feed_gain)]
    small_loads = [pltpu.make_async_copy(src, dst, load_sem.at[6 + i]) for i, (src, dst) in enumerate(small)]
    for load in loads + small_loads:
        load.start()

    barrier = pltpu.get_barrier_semaphore()
    for device in (at_x(x_next), at_x(x_prev), at_y(y_next), at_y(y_prev), at_z(z_next), at_z(z_prev), partner):
        pl.semaphore_signal(barrier, inc=1, device_id=device, device_id_type=mesh_type)
    with jax.named_scope("barrier"):
        pl.semaphore_wait(barrier, 7)

    def span(first, size, part):
        return pl.ds(first, size) if part is None else pl.ds(first + part * (size // 2), size // 2)

    def conv_piece(first, width):
        def view(what, yy, xx, colour, part):
            cols = span(first + colour * width, width, part)
            if what == "block":
                return conv_w.at[z_lo * SIDE + yy, of(0, xx, k_rows), cols]
            if what == "row":
                return conv_w.at[z_lo * SIDE + yy, :, cols]
            return conv_w.at[pl.ds(z_lo * SIDE, SIDE), of(0, xx, k_rows), cols]

        return view

    def up_piece(index):
        size = features // UP_PIECES // 2

        def view(what, yy, xx, colour, part):
            depth = span((2 * index + colour) * size, size, part)
            if what == "block":
                return up_w.at[yy, depth, of(0, xx, block)]
            if what == "row":
                return up_w.at[yy, depth, :]
            return up_w.at[:, depth, of(0, xx, block)]

        return view

    def split_cols(colour, which):
        width, first = DOWN_WIDTHS[SPLIT], DOWN_FIRST[SPLIT]
        return pl.ds(pl.multiple_of(2 * first + colour * width + which * (width // 2), 128), width // 2)

    def split_send(part):
        rows_of = pl.ds(part * 2, 2)
        for colour, device in ((0, at_z(z_next)), (1, at_z(z_prev))):
            src = down_w.at[rows_of, :, split_cols(colour, z_hi)]
            remote(src, relay.at[colour, rows_of], y_send.at[part], y_recv.at[part], device).start()

    def split_wait(number):
        both = relay.at[:, 0:2]
        pltpu.make_async_copy(both, both, y_recv.at[number]).wait()
        pltpu.make_async_copy(both, both, y_send.at[number]).wait()

    def split_pass(part):
        split_wait(part)
        rows_of = pl.ds(part * 2, 2)
        for colour, device, source in ((0, at_z(z_next), z_prev), (1, at_z(z_prev), z_next)):
            dst = down_w.at[rows_of, :, split_cols(colour, source // 2)]
            remote(relay.at[colour, rows_of], dst, y_send.at[2 + part], y_recv.at[2 + part], device).start()

    def down_piece(index):
        width, first = DOWN_WIDTHS[index], DOWN_FIRST[index]

        def view(what, yy, xx, colour, part):
            cols = pl.ds(2 * first + colour * width, width)
            if index == SPLIT:
                cols = split_cols(colour, z_hi)
            size = block if part is None else block // 2
            rows_of_block = pl.ds(pl.multiple_of(xx * block + (part or 0) * size, size), size)
            if what == "block":
                return down_w.at[yy, rows_of_block, cols]
            if what == "row":
                return down_w.at[yy, span(0, SIDE * block, part), cols]
            return down_w.at[:, rows_of_block, cols]

        return view

    views = [conv_piece(0, channels), conv_piece(2 * channels, channels // 2)]
    views += [up_piece(i) for i in range(UP_PIECES)] + [down_piece(i) for i in range(DOWN_PIECES)]

    def step_copies(piece, step):
        view = views[piece]
        if step == 0:
            own = [("block", y, x, 0, None), ("block", y, x, 1, None)]
            pairs = [(own[0], own[0]), (own[1], own[1])]
        elif step == 1:
            pairs = [
                (("block", y, x_prev, 0, 0), ("block", y, x_next, 0, 1)),
                (("block", y_prev, x, 1, 0), ("block", y_next, x, 1, 1)),
            ]
        elif step == 2:
            pairs = [(("row", y, x, 0, None),) * 2, (("col", y, x, 1, None),) * 2]
        else:
            pairs = [
                (("row", y_prev, x, 0, 0), ("row", y_next, x, 0, 1)),
                (("col", y, x_prev, 1, 0), ("col", y, x_next, 1, 1)),
            ]
        along_x = (at_x(x_next), at_x(x_prev))
        along_y = (at_y(y_next), at_y(y_prev))
        copies = []
        for colour in range(2):
            devices = along_x if (step < 2) == (colour == 0) else along_y
            for way in range(2):
                ref = view(*pairs[colour][way])
                copies.append(remote(ref, ref, send_sem.at[piece], recv_sem.at[piece * 4 + step], devices[way]))
        return copies

    flying = {}

    def z_copies(piece, stage):
        view = views[piece]
        sets = {
            0: [(("row", y, x, 0, None), ("col", y, x, 1, None))],
            1: [
                (("row", y_prev, x, 0, None), ("col", y, x_prev, 1, None)),
                (("row", y_next, x, 0, None), ("col", y, x_next, 1, None)),
            ],
            2: [(("row", lax.rem(y + 2, SIDE), x, 0, None), ("col", y, lax.rem(x + 2, SIDE), 1, None))],
        }[stage]
        copies = []
        for pair in sets:
            for colour in range(2):
                ref = view(*pair[colour])
                copies.append(remote(ref, ref, z_send.at[piece], z_recv.at[piece], at_z((z_next, z_prev)[colour])))
        return copies

    counts = {}

    def advance(piece):
        counts[piece] = counts.get(piece, 0) + 1
        step = 0
        if piece in flying:
            step = flying[piece]
            with jax.named_scope(f"wait_{piece}_{step}"):
                kib = int(4 * UNITS[piece] * 64 * (1, 0.5, 4, 2)[step])
                four = up_w.at[0, 0:kib, :]
                pltpu.make_async_copy(four, four, recv_sem.at[piece * 4 + step]).wait()
                pltpu.make_async_copy(four, four, send_sem.at[piece]).wait()
            step += 1
        if step < 4:
            copies = step_copies(piece, step)
            for copy in copies:
                copy.start()
            flying[piece] = step

    def z_go(piece, stage):
        for copy in z_copies(piece, stage):
            copy.start()

    def z_wait(piece):
        first = 2 * channels * piece
        whole = conv_w.at[pl.ds((1 - z_lo) * SIDE, SIDE), :, pl.ds(first, (2 - piece) * channels)]
        pltpu.make_async_copy(whole, whole, z_recv.at[piece]).wait()
        pltpu.make_async_copy(whole, whole, z_send.at[piece]).wait()

    ups = list(range(2, 2 + UP_PIECES))
    downs = list(range(2 + UP_PIECES, PIECES))

    def rms(src, dst, gain, first, count, step_rows=32):
        scale = gain[...]

        def body(i, carry):
            at = pl.ds(pl.multiple_of(i * step_rows, step_rows), step_rows)
            values = src[pl.ds(pl.multiple_of(first + i * step_rows, step_rows), step_rows), :].astype(F32)
            mean = jnp.sum(values * values, axis=1, keepdims=True) * (1.0 / features)
            dst[at, :] = (values * lax.rsqrt(mean + 1e-6) * scale).astype(BF16)
            return carry

        lax.fori_loop(0, count // step_rows, body, 0)

    mine = of(0, core, half)
    own, foreign = pl.ds(0, rows), pl.ds(rows, rows)
    low, high = pl.ds(0, part_rows), pl.ds(part_rows, part_rows)
    from_prev, from_next = pl.ds(rows, part_rows), pl.ds(rows + part_rows, part_rows)
    mix_send, mix_got = part.at[0, 0:rows, :], part_got.at[0:rows, :]
    x_swap = remote(x_hbm, x_full.at[:, mine], pair_send.at[0], pair_recv.at[0], partner)
    stat_swap = remote(stat_own, stat_got, pair_send.at[1], pair_recv.at[1], partner)
    mix_swap = remote(mix_send, mix_got, pair_send.at[2], pair_recv.at[2], partner)
    second_swap = remote(second.at[own, mine], second.at[own, mine], pair_send.at[3], pair_recv.at[3], partner)
    foreign_swap = remote(second.at[foreign, mine], second.at[foreign, mine], pair_send.at[4], pair_recv.at[4], partner)
    hops = [
        remote(second.at[low, mine], second.at[from_prev, mine], hop_send.at[0], hop_recv.at[0], at_z(z_next)),
        remote(second.at[high, mine], second.at[from_next, mine], hop_send.at[0], hop_recv.at[0], at_z(z_prev)),
    ]

    def first_norm():
        loads[4].wait()
        for load in small_loads:
            load.wait()
        x_swap.wait()
        rms(x_full, normed, mix_gain, 0, rows)
        padded[:, 0:32, :] = jnp.zeros((sequences, 32, channels), F32)

    tile = 256

    def plane_dot(which, cols):
        at = pl.ds(pl.multiple_of(which * half, half), half)
        weights = conv_w[pl.ds(which * SIDE, SIDE), :, cols].reshape(half, tile)
        return jnp.dot(normed[:, at], weights, preferred_element_type=F32)

    def value_gate_own():
        for n in range(2 * channels // tile):
            cols = slice(n * tile, (n + 1) * tile)
            own_sum[:, cols] = plane_dot(z_lo, cols)

    def value_gate_rest():
        for n in range(channels // tile):
            cols = slice(n * tile, (n + 1) * tile)
            gcols = slice(channels + n * tile, channels + (n + 1) * tile)
            value = own_sum[:, cols] + plane_dot(1 - z_lo, cols)
            gate = own_sum[:, gcols] + plane_dot(1 - z_lo, gcols)
            gated = value * jax.nn.sigmoid(gate)
            padded[:, 32 : 32 + LEN, cols] = gated.reshape(sequences, LEN, tile)

    def causal_filter():
        def body(s, carry):
            at = pl.ds(pl.multiple_of(s * LEN, LEN), LEN)
            first = jnp.zeros((LEN, 128), F32)
            square = jnp.zeros((LEN, 128), F32)
            for lane in range(channels // 128):
                cols = slice(lane * 128, (lane + 1) * 128)
                slab = padded[s, :, cols]
                total = jnp.broadcast_to(conv_bias[:, cols], (LEN, 128))
                for shift in range(8):
                    acc = None
                    for q in range(5):
                        k = 8 * q + shift - 2
                        if 0 <= k < KW:
                            tall = LEN + (8 if shift else 0)
                            term = taps[k : k + 1, cols] * slab[8 * q : 8 * q + tall]
                            acc = term if acc is None else acc + term
                    total = total + acc[shift : shift + LEN]
                filtered[at, cols] = total
                first = first + total
                square = square + total * total
            stat_own[0, at, :] = first
            stat_own[1, at, :] = square
            return carry

        lax.fori_loop(0, sequences, body, 0)
        stat_swap.start()

    def channel_norm():
        def body(i, carry):
            at = pl.ds(pl.multiple_of(i * 64, 64), 64)
            scale = 1.0 / (2 * channels)
            mean = jnp.sum(stat_own[0, at, :] + stat_got[0, at, :], axis=1, keepdims=True) * scale
            power = jnp.sum(stat_own[1, at, :] + stat_got[1, at, :], axis=1, keepdims=True) * scale
            spread = lax.rsqrt(power - mean * mean + 1e-5)
            centred = (filtered[at, :] - mean) * spread * chan_gain[...] + chan_bias[...]
            act[at, :] = (centred * jax.nn.sigmoid(centred)).astype(BF16)
            return carry

        lax.fori_loop(0, rows // 64, body, 0)

    def back_half(which):
        weights = conv_w[pl.ds(which * SIDE, SIDE), :, 2 * channels : 3 * channels].reshape(half, channels)
        return lax.dot_general(act[...], weights, (((1,), (1,)), ((), ())), preferred_element_type=F32)

    def back_other():
        mix_send[...] = back_half(other).astype(BF16)
        mix_swap.start()

    def back_own():
        own_sum[...] = back_half(core)

    def residual():
        mixed = own_sum[...].astype(BF16).astype(F32) + mix_got[...].astype(F32)
        second[own, mine] = (x_full[:, mine].astype(F32) + mixed).astype(BF16)
        for hop in hops:
            hop.start()
        second_swap.start()

    def up(source, first, begin, end):
        at = pl.ds(first, rows)

        def body(i, carry):
            product = jnp.dot(source[...], up_w[i], preferred_element_type=F32)
            positive = jnp.maximum(product, 0.0)
            hidden[at, pl.ds(pl.multiple_of(i * SIDE * block, SIDE * block), SIDE * block)] = (positive * positive).astype(BF16)
            return carry

        lax.fori_loop(begin, end, body, 0)

    def arrived():
        both = second.at[foreign, mine]
        pltpu.make_async_copy(both, both, hop_recv.at[0]).wait()
        pltpu.make_async_copy(both, both, hop_send.at[0]).wait()
        foreign_swap.start()

    swaps = {}

    def down(index):
        width, first = DOWN_WIDTHS[index], DOWN_FIRST[index]
        cols = pl.ds(first, width)
        depth = SIDE * SIDE * block
        swaps[index] = []
        for number, at in enumerate((foreign, own)):

            def body(i, carry):
                chunk = pl.ds(pl.multiple_of(at.start + i * part_rows, part_rows), part_rows)
                weights = down_w[:, :, pl.ds(2 * first, 2 * width)].reshape(depth, 2 * width)
                product = jnp.dot(hidden[chunk, :], weights, preferred_element_type=F32).astype(BF16)
                part[0, chunk, cols] = product[:, :width]
                part[1, chunk, cols] = product[:, width:]
                return carry

            lax.fori_loop(0, 2, body, 0)
            slot = 5 + 2 * index + number
            swap = remote(part.at[other, at, cols], part_got.at[at, cols], pair_send.at[5 if number == 0 else 6 + index % 2], pair_recv.at[slot], partner)
            swap.start()
            swaps[index].append(swap)

    def send_back(index):
        width, first = DOWN_WIDTHS[index], DOWN_FIRST[index]
        cols = pl.ds(first, width)
        swaps[index][0].wait()
        ret_send[:, cols] = (part[core, foreign, cols].astype(F32) + part_got[foreign, cols].astype(F32)).astype(BF16)
        for at, device in ((low, at_z(z_prev)), (high, at_z(z_next))):
            slot = 1 + index
            back = remote(ret_send.at[at, cols], ret_got.at[at, cols], hop_send.at[slot], hop_recv.at[slot], device)
            back.start()

    def sum_own(index):
        width, first = DOWN_WIDTHS[index], DOWN_FIRST[index]
        cols = pl.ds(first, width)
        swaps[index][1].wait()
        there = pl.ds(pl.multiple_of(core * half + first, 128), width)
        own_sum[:, cols] = (
            second[own, there].astype(F32) + part[core, own, cols].astype(F32) + part_got[own, cols].astype(F32)
        )

    def finish(index):
        width, first = DOWN_WIDTHS[index], DOWN_FIRST[index]
        cols = pl.ds(first, width)
        both = ret_got.at[:, cols]
        pltpu.make_async_copy(both, both, hop_recv.at[1 + index]).wait()
        pltpu.make_async_copy(both, both, hop_send.at[1 + index]).wait()
        out_vmem[:, cols] = (own_sum[:, cols] + ret_got[:, cols].astype(F32)).astype(BF16)

    def down_step(index):
        if index == SPLIT:
            split_wait(2)
            split_wait(3)
        down(index)
        send_back(index)
        if index:
            sum_own(index - 1)
        if index > 1:
            finish(index - 2)

    actions = dict(
        rmsx=first_norm,
        vg0=value_gate_own,
        zw0=lambda: z_wait(0),
        vg1=value_gate_rest,
        filter=causal_filter,
        statw=stat_swap.wait,
        chan=channel_norm,
        zw1=lambda: z_wait(1),
        bo=back_other,
        bw=back_own,
        mixw=mix_swap.wait,
        second=residual,
        secw=second_swap.wait,
        rms=lambda: rms(second, normed, feed_gain, 0, rows),
        upa=lambda: up(normed, 0, 0, SIDE // 2),
        upb=lambda: up(normed, 0, SIDE // 2, SIDE),
        hopw=arrived,
        forw=foreign_swap.wait,
        rmsf=lambda: rms(second, x_full, feed_gain, rows, rows),
        upfa=lambda: up(x_full, rows, 0, SIDE // 2),
        upfb=lambda: up(x_full, rows, SIDE // 2, SIDE),
    )
    for index in range(DOWN_PIECES):
        actions[f"down{index}"] = functools.partial(down_step, index)

    first_load = {0: (0, 1), 1: (2,)}
    first_load.update({piece: (3,) for piece in ups})
    first_load.update({piece: (6 if i == SPLIT else 5,) for i, piece in enumerate(downs)})
    split_width = DOWN_WIDTHS[SPLIT]
    most = down_w.at[y, of(0, x, block), 0 : features - 2 * split_width]
    few = down_w.at[y, of(0, x, block), 0:split_width]
    loads[5:] = [pltpu.make_async_copy(most, most, load_sem.at[5]), pltpu.make_async_copy(few, few, load_sem.at[12])]
    loaded = set()

    x_swap.start()
    for name in ORDER:
        if name[0] == "a" and name[1:].isdigit():
            piece = int(name[1:])
            for number in first_load[piece]:
                if number not in loaded:
                    loads[number].wait()
                    loaded.add(number)
            advance(piece)
        elif name[0] == "y":
            number = int(name[1:])
            with jax.named_scope(name):
                (split_send if number < 2 else split_pass)(number % 2)
        elif name[0] == "z" and name[1:].isdigit():
            z_go(int(name[1]), int(name[2]))
        else:
            with jax.named_scope(name):
                actions[name]()

    sum_own(DOWN_PIECES - 1)
    finish(DOWN_PIECES - 2)
    with jax.named_scope("last"):
        finish(DOWN_PIECES - 1)
    assert all(counts[piece] == 5 for piece in range(PIECES)), counts


def shards(
    hidden_in, mix_gain, w_value, w_gate, conv_taps, conv_bias, chan_gain, chan_bias, w_back, feed_gain, w_up, w_down
):
    rows, half = hidden_in.shape
    features = 2 * half
    channels = w_value.shape[1]
    block = w_up.shape[1]
    plane = SIDE * SIDE
    sequences = rows // LEN
    vmem = pl.BlockSpec(memory_space=pltpu.VMEM)
    hbm = pl.BlockSpec(memory_space=pl.ANY)
    dma = pltpu.SemaphoreType.DMA
    scratch = [
        pltpu.VMEM((2 * SIDE, SIDE * w_value.shape[0], 3 * channels), BF16),
        pltpu.VMEM((SIDE, features, SIDE * block), BF16),
        pltpu.VMEM((SIDE, SIDE * block, features), BF16),
        pltpu.VMEM((rows, features), BF16),
        pltpu.VMEM((rows, features), BF16),
        pltpu.VMEM((sequences, 32 + LEN, channels), F32),
        pltpu.VMEM((rows, channels), F32),
        pltpu.VMEM((rows, channels), BF16),
        pltpu.VMEM((2, rows, 128), F32),
        pltpu.VMEM((2, rows, 128), F32),
        pltpu.VMEM((1, features), F32),
        pltpu.VMEM(conv_taps.shape, F32),
        pltpu.VMEM((1, channels), F32),
        pltpu.VMEM((1, channels), F32),
        pltpu.VMEM((1, channels), F32),
        pltpu.VMEM((1, features), F32),
        pltpu.VMEM((2 * rows, features), BF16),
        pltpu.VMEM((2 * rows, plane * block), BF16),
        pltpu.VMEM((2, 2 * rows, half), BF16),
        pltpu.VMEM((2 * rows, half), BF16),
        pltpu.VMEM((rows, half), F32),
        pltpu.VMEM((rows, half), BF16),
        pltpu.VMEM((rows, half), BF16),
        pltpu.VMEM((2, SIDE, SIDE * block, DOWN_WIDTHS[SPLIT] // 2), BF16),
        dma((13,)),
        dma((PIECES,)),
        dma((PIECES * 4,)),
        dma((2,)),
        dma((2,)),
        dma((8,)),
        dma((5 + 2 * DOWN_PIECES,)),
        dma((1 + DOWN_PIECES,)),
        dma((1 + DOWN_PIECES,)),
        dma((4,)),
        dma((4,)),
    ]
    return pl.pallas_call(
        kernel,
        out_shape=pltpu.VMEM((rows, half), BF16),
        in_specs=[hbm] * 12,
        out_specs=vmem,
        scratch_shapes=scratch,
        compiler_params=pltpu.CompilerParams(
            collective_id=0, has_side_effects=True, vmem_limit_bytes=61 * 2**20
        ),
    )(
        hidden_in,
        mix_gain[None, :],
        w_value,
        w_gate,
        conv_taps,
        conv_bias[None, :],
        chan_gain[None, :],
        chan_bias[None, :],
        w_back.T,
        feed_gain[None, :],
        w_up,
        w_down,
    )


def solution(mesh):
    placed = (
        P(("rep", "fs"), "tp"),
        P(),
        P("fs", "tp"),
        P("fs", "tp"),
        P(None, "tp"),
        P("tp"),
        P("tp"),
        P("tp"),
        P("tp", "fs"),
        P(),
        P(None, ("fs", "tp")),
        P(("fs", "tp"), None),
    )
    return jax.shard_map(
        shards, mesh=mesh, in_specs=placed, out_specs=P(("rep", "fs"), "tp"), check_vma=False
    )
```

```python
import functools

import jax
import jax.numpy as jnp
from jax import lax
from jax.experimental import pallas as pl
from jax.experimental.pallas import tpu as pltpu
from jax.sharding import PartitionSpec as P

KW = 31
LEN = 128
SIDE = 4
F32 = jnp.float32
BF16 = jnp.bfloat16
UP_PIECES = 4
SPLIT = 0
DOWN_WIDTHS = (256, 256, 256, 128, 128)
DOWN_FIRST = (0, 256, 512, 768, 896)
DOWN_PIECES = len(DOWN_WIDTHS)
PIECES = 2 + UP_PIECES + DOWN_PIECES
UNITS = (1, 0.5) + (4 / UP_PIECES,) * UP_PIECES
UNITS += tuple(width / 256 / (2 if i == SPLIT else 1) for i, width in enumerate(DOWN_WIDTHS))

ORDER = (
    "a0", "a5", "a1", "a6", "a8", "a0", "a10", "a3", "a1", "a7", "a5", "a0", "rmsx", "a3", "a1", "a6", "z10", "z00",
    "a9", "a0", "z01", "a4", "a6", "a10", "a1", "a2", "a3", "a0", "z02", "a6", "vg0", "z11", "a1", "a2", "a4", "a5",
    "a7", "z12", "a6", "a3", "zw0", "vg1", "a4", "y0", "filter", "y1", "a2", "statw", "chan", "a5", "zw1", "bo",
    "a8", "bw", "mixw", "second", "a4", "a2", "secw", "y2", "rms0", "a7", "a5", "a3", "rms1", "hopw0", "a8", "a4",
    "a9", "a2", "forw0", "rmsf0", "upf00", "upf01", "hopw1", "y3", "a7", "up0", "up1", "forw1", "a10", "rmsf1",
    "upf10", "a9", "upf11", "a8", "dF0", "up2", "sb0", "a7", "up3", "dF1", "a9", "a10", "dO0", "sb1", "a8", "dF2",
    "dO1", "sb2", "a9", "dF3", "dO2", "sb3", "a10", "dF4", "dO3", "sb4", "dO4",
)


def kernel(
    x_hbm, mix_gain_hbm, wv_hbm, wg_hbm, taps_hbm, conv_bias_hbm, chan_gain_hbm, chan_bias_hbm, wb_hbm,
    feed_gain_hbm, wu_hbm, wd_hbm,
    out_vmem,
    conv_w, up_w, down_w, x_full, normed, padded, filtered, act, stat_own, stat_got,
    mix_gain, taps, conv_bias, chan_gain, chan_bias, feed_gain,
    second, hidden, part, part_got, own_sum, ret_send, ret_got,
    relay, load_sem, send_sem, recv_sem, z_send, z_recv, pair_send, pair_recv, hop_send, hop_recv, y_send, y_recv,
):
    rows, half = x_hbm.shape
    features = 2 * half
    channels = wv_hbm.shape[1]
    k_rows = wv_hbm.shape[0]
    block = wu_hbm.shape[1]
    sequences = rows // LEN
    part_rows = rows // 2

    core = lax.axis_index("tp")
    other = 1 - core
    place = lax.axis_index("fs")
    z_hi = lax.axis_index("rep")
    x = lax.rem(place, SIDE)
    y = lax.rem(place // SIDE, SIDE)
    z_lo = place // (SIDE * SIDE)
    z = z_hi * 2 + z_lo
    x_next, x_prev = lax.rem(x + 1, SIDE), lax.rem(x + SIDE - 1, SIDE)
    y_next, y_prev = lax.rem(y + 1, SIDE), lax.rem(y + SIDE - 1, SIDE)
    z_next, z_prev = lax.rem(z + 1, 4), lax.rem(z + 3, 4)

    def at_x(xx):
        return {"fs": z_lo * SIDE * SIDE + y * SIDE + xx}

    def at_y(yy):
        return {"fs": z_lo * SIDE * SIDE + yy * SIDE + x}

    def at_z(zz):
        return {"rep": zz // 2, "fs": lax.rem(zz, 2) * SIDE * SIDE + y * SIDE + x}

    partner = {"tp": other}
    mesh_type = pl.DeviceIdType.MESH

    def remote(src, dst, send, recv, device):
        return pltpu.make_async_remote_copy(
            src_ref=src, dst_ref=dst, send_sem=send, recv_sem=recv, device_id=device, device_id_type=mesh_type
        )

    def of(ref, i, n):
        return pl.ds(pl.multiple_of(i * n, n), n)

    conv_row = z_lo * SIDE + y
    loads = [
        pltpu.make_async_copy(wv_hbm, conv_w.at[conv_row, of(0, x, k_rows), 0:channels], load_sem.at[0]),
        pltpu.make_async_copy(wg_hbm, conv_w.at[conv_row, of(0, x, k_rows), channels : 2 * channels], load_sem.at[1]),
        pltpu.make_async_copy(wb_hbm, conv_w.at[conv_row, of(0, x, k_rows), 2 * channels : 3 * channels], load_sem.at[2]),
        pltpu.make_async_copy(wu_hbm, up_w.at[y, :, of(0, x, block)], load_sem.at[3]),
        pltpu.make_async_copy(x_hbm, x_full.at[:, of(0, core, half)], load_sem.at[4]),
    ]
    for index in range(DOWN_PIECES):
        width, first = DOWN_WIDTHS[index], DOWN_FIRST[index]
        for h in range(2):
            size, shift, sem = width, 0, 5
            if index == SPLIT:
                size, sem = width // 2, 12
                shift = z_hi * size
            src = wd_hbm.at[:, pl.ds(pl.multiple_of(h * half + first + shift, 128), size)]
            dst = down_w.at[y, of(0, x, block), pl.ds(pl.multiple_of(2 * first + h * width + shift, 128), size)]
            loads.append(pltpu.make_async_copy(src, dst, load_sem.at[sem]))
    small = [(mix_gain_hbm, mix_gain), (taps_hbm, taps), (conv_bias_hbm, conv_bias)]
    small += [(chan_gain_hbm, chan_gain), (chan_bias_hbm, chan_bias), (feed_gain_hbm, feed_gain)]
    small_loads = [pltpu.make_async_copy(src, dst, load_sem.at[6 + i]) for i, (src, dst) in enumerate(small)]
    for load in loads + small_loads:
        load.start()

    barrier = pltpu.get_barrier_semaphore()
    for device in (at_x(x_next), at_x(x_prev), at_y(y_next), at_y(y_prev), at_z(z_next), at_z(z_prev), partner):
        pl.semaphore_signal(barrier, inc=1, device_id=device, device_id_type=mesh_type)
    with jax.named_scope("barrier"):
        pl.semaphore_wait(barrier, 7)

    def span(first, size, part):
        return pl.ds(first, size) if part is None else pl.ds(first + part * (size // 2), size // 2)

    def conv_piece(first, width):
        def view(what, yy, xx, colour, part):
            cols = span(first + colour * width, width, part)
            if what == "block":
                return conv_w.at[z_lo * SIDE + yy, of(0, xx, k_rows), cols]
            if what == "row":
                return conv_w.at[z_lo * SIDE + yy, :, cols]
            return conv_w.at[pl.ds(z_lo * SIDE, SIDE), of(0, xx, k_rows), cols]

        return view

    def up_piece(index):
        size = features // UP_PIECES // 2

        def view(what, yy, xx, colour, part):
            depth = span((2 * index + colour) * size, size, part)
            if what == "block":
                return up_w.at[yy, depth, of(0, xx, block)]
            if what == "row":
                return up_w.at[yy, depth, :]
            return up_w.at[:, depth, of(0, xx, block)]

        return view

    def split_cols(colour, which):
        width, first = DOWN_WIDTHS[SPLIT], DOWN_FIRST[SPLIT]
        return pl.ds(pl.multiple_of(2 * first + colour * width + which * (width // 2), 128), width // 2)

    def split_send(part):
        rows_of = pl.ds(part * 2, 2)
        for colour, device in ((0, at_z(z_next)), (1, at_z(z_prev))):
            src = down_w.at[rows_of, :, split_cols(colour, z_hi)]
            remote(src, relay.at[colour, rows_of], y_send.at[part], y_recv.at[part], device).start()

    def split_wait(number):
        both = relay.at[:, 0:2]
        pltpu.make_async_copy(both, both, y_recv.at[number]).wait()
        pltpu.make_async_copy(both, both, y_send.at[number]).wait()

    def split_pass(part):
        split_wait(part)
        rows_of = pl.ds(part * 2, 2)
        for colour, device, source in ((0, at_z(z_next), z_prev), (1, at_z(z_prev), z_next)):
            dst = down_w.at[rows_of, :, split_cols(colour, source // 2)]
            remote(relay.at[colour, rows_of], dst, y_send.at[2 + part], y_recv.at[2 + part], device).start()

    def down_piece(index):
        width, first = DOWN_WIDTHS[index], DOWN_FIRST[index]

        def view(what, yy, xx, colour, part):
            cols = pl.ds(2 * first + colour * width, width)
            if index == SPLIT:
                cols = split_cols(colour, z_hi)
            size = block if part is None else block // 2
            rows_of_block = pl.ds(pl.multiple_of(xx * block + (part or 0) * size, size), size)
            if what == "block":
                return down_w.at[yy, rows_of_block, cols]
            if what == "row":
                return down_w.at[yy, span(0, SIDE * block, part), cols]
            return down_w.at[:, rows_of_block, cols]

        return view

    views = [conv_piece(0, channels), conv_piece(2 * channels, channels // 2)]
    views += [up_piece(i) for i in range(UP_PIECES)] + [down_piece(i) for i in range(DOWN_PIECES)]

    def step_copies(piece, step):
        view = views[piece]
        if step == 0:
            own = [("block", y, x, 0, None), ("block", y, x, 1, None)]
            pairs = [(own[0], own[0]), (own[1], own[1])]
        elif step == 1:
            pairs = [
                (("block", y, x_prev, 0, 0), ("block", y, x_next, 0, 1)),
                (("block", y_prev, x, 1, 0), ("block", y_next, x, 1, 1)),
            ]
        elif step == 2:
            pairs = [(("row", y, x, 0, None),) * 2, (("col", y, x, 1, None),) * 2]
        else:
            pairs = [
                (("row", y_prev, x, 0, 0), ("row", y_next, x, 0, 1)),
                (("col", y, x_prev, 1, 0), ("col", y, x_next, 1, 1)),
            ]
        along_x = (at_x(x_next), at_x(x_prev))
        along_y = (at_y(y_next), at_y(y_prev))
        copies = []
        for colour in range(2):
            devices = along_x if (step < 2) == (colour == 0) else along_y
            for way in range(2):
                ref = view(*pairs[colour][way])
                copies.append(remote(ref, ref, send_sem.at[piece], recv_sem.at[piece * 4 + step], devices[way]))
        return copies

    flying = {}

    def z_copies(piece, stage):
        view = views[piece]
        sets = {
            0: [(("row", y, x, 0, None), ("col", y, x, 1, None))],
            1: [
                (("row", y_prev, x, 0, None), ("col", y, x_prev, 1, None)),
                (("row", y_next, x, 0, None), ("col", y, x_next, 1, None)),
            ],
            2: [(("row", lax.rem(y + 2, SIDE), x, 0, None), ("col", y, lax.rem(x + 2, SIDE), 1, None))],
        }[stage]
        copies = []
        for pair in sets:
            for colour in range(2):
                ref = view(*pair[colour])
                copies.append(remote(ref, ref, z_send.at[piece], z_recv.at[piece], at_z((z_next, z_prev)[colour])))
        return copies

    counts = {}

    def advance(piece):
        counts[piece] = counts.get(piece, 0) + 1
        step = 0
        if piece in flying:
            step = flying[piece]
            with jax.named_scope(f"wait_{piece}_{step}"):
                kib = int(4 * UNITS[piece] * 64 * (1, 0.5, 4, 2)[step])
                four = up_w.at[0, 0:kib, :]
                pltpu.make_async_copy(four, four, recv_sem.at[piece * 4 + step]).wait()
                pltpu.make_async_copy(four, four, send_sem.at[piece]).wait()
            step += 1
        if step < 4:
            copies = step_copies(piece, step)
            for copy in copies:
                copy.start()
            flying[piece] = step

    def z_go(piece, stage):
        for copy in z_copies(piece, stage):
            copy.start()

    def z_wait(piece):
        first = 2 * channels * piece
        whole = conv_w.at[pl.ds((1 - z_lo) * SIDE, SIDE), :, pl.ds(first, (2 - piece) * channels)]
        pltpu.make_async_copy(whole, whole, z_recv.at[piece]).wait()
        pltpu.make_async_copy(whole, whole, z_send.at[piece]).wait()

    ups = list(range(2, 2 + UP_PIECES))
    downs = list(range(2 + UP_PIECES, PIECES))

    def rms(src, dst, gain, first, count, step_rows=32, to=0):
        scale = gain[...]

        def body(i, carry):
            at = pl.ds(pl.multiple_of(to + i * step_rows, step_rows), step_rows)
            values = src[pl.ds(pl.multiple_of(first + i * step_rows, step_rows), step_rows), :].astype(F32)
            mean = jnp.sum(values * values, axis=1, keepdims=True) * (1.0 / features)
            dst[at, :] = (values * lax.rsqrt(mean + 1e-6) * scale).astype(BF16)
            return carry

        lax.fori_loop(0, count // step_rows, body, 0)

    mine = of(0, core, half)
    own, foreign = pl.ds(0, rows), pl.ds(rows, rows)
    mix_send, mix_got = part.at[0, 0:rows, :], part_got.at[0:rows, :]
    x_swap = remote(x_hbm, x_full.at[:, mine], pair_send.at[0], pair_recv.at[0], partner)
    stat_swap = remote(stat_own, stat_got, pair_send.at[1], pair_recv.at[1], partner)
    mix_swap = remote(mix_send, mix_got, pair_send.at[2], pair_recv.at[2], partner)
    second_swap = remote(second.at[own, mine], second.at[own, mine], pair_send.at[3], pair_recv.at[3], partner)
    part_rows, strip = rows // 2, rows // 4

    def strip_of(first, k, way):
        return pl.ds(first + k * part_rows + way * strip, strip)

    def home_of(k, way):
        return pl.ds(way * part_rows + k * strip, strip)

    far = [second.at[pl.ds(rows + k * part_rows, part_rows), mine] for k in range(2)]
    foreign_swap = [remote(far[k], far[k], pair_send.at[4 + k], pair_recv.at[4 + k], partner) for k in range(2)]
    hops = [
        remote(
            second.at[home_of(k, way), mine], second.at[strip_of(rows, k, way), mine],
            hop_send.at[k], hop_recv.at[k], at_z((z_next, z_prev)[way]),
        )
        for k in range(2)
        for way in range(2)
    ]

    def first_norm():
        loads[4].wait()
        for load in small_loads:
            load.wait()
        x_swap.wait()
        rms(x_full, normed, mix_gain, 0, rows)
        padded[:, 0:32, :] = jnp.zeros((sequences, 32, channels), F32)

    tile = 256

    def plane_dot(which, cols):
        at = pl.ds(pl.multiple_of(which * half, half), half)
        weights = conv_w[pl.ds(which * SIDE, SIDE), :, cols].reshape(half, tile)
        return jnp.dot(normed[:, at], weights, preferred_element_type=F32)

    def value_gate_own():
        for n in range(2 * channels // tile):
            cols = slice(n * tile, (n + 1) * tile)
            own_sum[:, cols] = plane_dot(z_lo, cols)

    def value_gate_rest():
        for n in range(channels // tile):
            cols = slice(n * tile, (n + 1) * tile)
            gcols = slice(channels + n * tile, channels + (n + 1) * tile)
            value = own_sum[:, cols] + plane_dot(1 - z_lo, cols)
            gate = own_sum[:, gcols] + plane_dot(1 - z_lo, gcols)
            gated = value * jax.nn.sigmoid(gate)
            padded[:, 32 : 32 + LEN, cols] = gated.reshape(sequences, LEN, tile)

    def causal_filter():
        def body(s, carry):
            at = pl.ds(pl.multiple_of(s * LEN, LEN), LEN)
            first = jnp.zeros((LEN, 128), F32)
            square = jnp.zeros((LEN, 128), F32)
            for lane in range(channels // 128):
                cols = slice(lane * 128, (lane + 1) * 128)
                slab = padded[s, :, cols]
                total = jnp.broadcast_to(conv_bias[:, cols], (LEN, 128))
                for shift in range(8):
                    acc = None
                    for q in range(5):
                        k = 8 * q + shift - 2
                        if 0 <= k < KW:
                            tall = LEN + (8 if shift else 0)
                            term = taps[k : k + 1, cols] * slab[8 * q : 8 * q + tall]
                            acc = term if acc is None else acc + term
                    total = total + acc[shift : shift + LEN]
                filtered[at, cols] = total
                first = first + total
                square = square + total * total
            stat_own[0, at, :] = first
            stat_own[1, at, :] = square
            return carry

        lax.fori_loop(0, sequences, body, 0)
        stat_swap.start()

    def channel_norm():
        def body(i, carry):
            at = pl.ds(pl.multiple_of(i * 64, 64), 64)
            scale = 1.0 / (2 * channels)
            mean = jnp.sum(stat_own[0, at, :] + stat_got[0, at, :], axis=1, keepdims=True) * scale
            power = jnp.sum(stat_own[1, at, :] + stat_got[1, at, :], axis=1, keepdims=True) * scale
            spread = lax.rsqrt(power - mean * mean + 1e-5)
            centred = (filtered[at, :] - mean) * spread * chan_gain[...] + chan_bias[...]
            act[at, :] = (centred * jax.nn.sigmoid(centred)).astype(BF16)
            return carry

        lax.fori_loop(0, rows // 64, body, 0)

    def back_half(which):
        weights = conv_w[pl.ds(which * SIDE, SIDE), :, 2 * channels : 3 * channels].reshape(half, channels)
        return lax.dot_general(act[...], weights, (((1,), (1,)), ((), ())), preferred_element_type=F32)

    def back_other():
        mix_send[...] = back_half(other).astype(BF16)
        mix_swap.start()

    def back_own():
        own_sum[...] = back_half(core)

    def residual():
        mixed = own_sum[...].astype(BF16).astype(F32) + mix_got[...].astype(F32)
        second[own, mine] = (x_full[:, mine].astype(F32) + mixed).astype(BF16)
        for hop in hops:
            hop.start()
        second_swap.start()

    def up(source, first, begin, end):
        at = pl.ds(first, source.shape[0])

        def body(i, carry):
            product = jnp.dot(source[...], up_w[i], preferred_element_type=F32)
            positive = jnp.maximum(product, 0.0)
            hidden[at, pl.ds(pl.multiple_of(i * SIDE * block, SIDE * block), SIDE * block)] = (positive * positive).astype(BF16)
            return carry

        lax.fori_loop(begin, end, body, 0)

    def arrived(k):
        pltpu.make_async_copy(far[k], far[k], hop_recv.at[k]).wait()
        pltpu.make_async_copy(far[k], far[k], hop_send.at[k]).wait()
        foreign_swap[k].start()

    def far_norm(k):
        rms(second, x_full, feed_gain, rows + k * part_rows, part_rows, to=k * part_rows)

    def far_up(k, begin):
        up(x_full.at[pl.ds(k * part_rows, part_rows), :], rows + k * part_rows, begin, begin + SIDE // 2)

    swaps = {}

    def down(index, number):
        width, first = DOWN_WIDTHS[index], DOWN_FIRST[index]
        cols = pl.ds(first, width)
        depth = SIDE * SIDE * block
        at = (foreign, own)[number]
        many = 1 if width >= 256 else 2
        if index == SPLIT and number == 0:
            split_wait(2)
            split_wait(3)

        def body(i, carry):
            chunk = pl.ds(pl.multiple_of(at.start + i * (rows // many), rows // many), rows // many)
            weights = down_w[:, :, pl.ds(2 * first, 2 * width)].reshape(depth, 2 * width)
            product = jnp.dot(hidden[chunk, :], weights, preferred_element_type=F32).astype(BF16)
            part[0, chunk, cols] = product[:, :width]
            part[1, chunk, cols] = product[:, width:]
            return carry

        lax.fori_loop(0, many, body, 0)
        sem = pair_send.at[6 + number * (1 + index)]
        swap = remote(part.at[other, at, cols], part_got.at[at, cols], sem, pair_recv.at[6 + 2 * index + number], partner)
        swap.start()
        swaps[index, number] = swap

    def send_back(index):
        width, first = DOWN_WIDTHS[index], DOWN_FIRST[index]
        cols = pl.ds(first, width)
        swaps[index, 0].wait()
        ret_send[:, cols] = (part[core, foreign, cols].astype(F32) + part_got[foreign, cols].astype(F32)).astype(BF16)
        for k in range(2):
            for way, device in ((0, at_z(z_prev)), (1, at_z(z_next))):
                src, dst = ret_send.at[strip_of(0, k, way), cols], ret_got.at[home_of(k, way), cols]
                remote(src, dst, hop_send.at[2 + index], hop_recv.at[2 + index], device).start()

    def finish(index):
        width, first = DOWN_WIDTHS[index], DOWN_FIRST[index]
        cols = pl.ds(first, width)
        swaps[index, 1].wait()
        both = ret_got.at[:, cols]
        pltpu.make_async_copy(both, both, hop_recv.at[2 + index]).wait()
        pltpu.make_async_copy(both, both, hop_send.at[2 + index]).wait()
        there = pl.ds(pl.multiple_of(core * half + first, 128), width)
        total = second[own, there].astype(F32) + part[core, own, cols].astype(F32) + part_got[own, cols].astype(F32)
        out_vmem[:, cols] = (total + ret_got[:, cols].astype(F32)).astype(BF16)

    actions = dict(
        rmsx=first_norm,
        vg0=value_gate_own,
        zw0=lambda: z_wait(0),
        vg1=value_gate_rest,
        filter=causal_filter,
        statw=stat_swap.wait,
        chan=channel_norm,
        zw1=lambda: z_wait(1),
        bo=back_other,
        bw=back_own,
        mixw=mix_swap.wait,
        second=residual,
        secw=second_swap.wait,
        rms0=lambda: rms(second, normed, feed_gain, 0, part_rows),
        rms1=lambda: rms(second, normed, feed_gain, part_rows, part_rows, to=part_rows),
        hopw0=lambda: arrived(0),
        hopw1=lambda: arrived(1),
        forw0=foreign_swap[0].wait,
        forw1=foreign_swap[1].wait,
        rmsf0=lambda: far_norm(0),
        rmsf1=lambda: far_norm(1),
    )
    for index in range(SIDE):
        actions[f"up{index}"] = functools.partial(up, normed, 0, index, index + 1)
    for k in range(2):
        for index in range(2):
            actions[f"upf{k}{index}"] = functools.partial(far_up, k, 2 * index)
    for index in range(DOWN_PIECES):
        actions[f"dF{index}"] = functools.partial(down, index, 0)
        actions[f"dO{index}"] = functools.partial(down, index, 1)
        actions[f"sb{index}"] = functools.partial(send_back, index)

    first_load = {0: (0, 1), 1: (2,)}
    first_load.update({piece: (3,) for piece in ups})
    first_load.update({piece: (6 if i == SPLIT else 5,) for i, piece in enumerate(downs)})
    split_width = DOWN_WIDTHS[SPLIT]
    most = down_w.at[y, of(0, x, block), 0 : features - 2 * split_width]
    few = down_w.at[y, of(0, x, block), 0:split_width]
    loads[5:] = [pltpu.make_async_copy(most, most, load_sem.at[5]), pltpu.make_async_copy(few, few, load_sem.at[12])]
    loaded = set()

    x_swap.start()
    for name in ORDER:
        if name[0] == "a" and name[1:].isdigit():
            piece = int(name[1:])
            for number in first_load[piece]:
                if number not in loaded:
                    loads[number].wait()
                    loaded.add(number)
            advance(piece)
        elif name[0] == "y":
            number = int(name[1:])
            with jax.named_scope(name):
                (split_send if number < 2 else split_pass)(number % 2)
        elif name[0] == "z" and name[1:].isdigit():
            z_go(int(name[1]), int(name[2]))
        else:
            with jax.named_scope(name):
                actions[name]()

    for index in range(DOWN_PIECES):
        with jax.named_scope(f"finish{index}"):
            finish(index)
    assert all(counts[piece] == 5 for piece in range(PIECES)), counts


def shards(
    hidden_in, mix_gain, w_value, w_gate, conv_taps, conv_bias, chan_gain, chan_bias, w_back, feed_gain, w_up, w_down
):
    rows, half = hidden_in.shape
    features = 2 * half
    channels = w_value.shape[1]
    block = w_up.shape[1]
    plane = SIDE * SIDE
    sequences = rows // LEN
    vmem = pl.BlockSpec(memory_space=pltpu.VMEM)
    hbm = pl.BlockSpec(memory_space=pl.ANY)
    dma = pltpu.SemaphoreType.DMA
    scratch = [
        pltpu.VMEM((2 * SIDE, SIDE * w_value.shape[0], 3 * channels), BF16),
        pltpu.VMEM((SIDE, features, SIDE * block), BF16),
        pltpu.VMEM((SIDE, SIDE * block, features), BF16),
        pltpu.VMEM((rows, features), BF16),
        pltpu.VMEM((rows, features), BF16),
        pltpu.VMEM((sequences, 32 + LEN, channels), F32),
        pltpu.VMEM((rows, channels), F32),
        pltpu.VMEM((rows, channels), BF16),
        pltpu.VMEM((2, rows, 128), F32),
        pltpu.VMEM((2, rows, 128), F32),
        pltpu.VMEM((1, features), F32),
        pltpu.VMEM(conv_taps.shape, F32),
        pltpu.VMEM((1, channels), F32),
        pltpu.VMEM((1, channels), F32),
        pltpu.VMEM((1, channels), F32),
        pltpu.VMEM((1, features), F32),
        pltpu.VMEM((2 * rows, features), BF16),
        pltpu.VMEM((2 * rows, plane * block), BF16),
        pltpu.VMEM((2, 2 * rows, half), BF16),
        pltpu.VMEM((2 * rows, half), BF16),
        pltpu.VMEM((rows, half), F32),
        pltpu.VMEM((rows, half), BF16),
        pltpu.VMEM((rows, half), BF16),
        pltpu.VMEM((2, SIDE, SIDE * block, DOWN_WIDTHS[SPLIT] // 2), BF16),
        dma((13,)),
        dma((PIECES,)),
        dma((PIECES * 4,)),
        dma((2,)),
        dma((2,)),
        dma((7 + DOWN_PIECES,)),
        dma((6 + 2 * DOWN_PIECES,)),
        dma((2 + DOWN_PIECES,)),
        dma((2 + DOWN_PIECES,)),
        dma((4,)),
        dma((4,)),
    ]
    return pl.pallas_call(
        kernel,
        out_shape=pltpu.VMEM((rows, half), BF16),
        in_specs=[hbm] * 12,
        out_specs=vmem,
        scratch_shapes=scratch,
        compiler_params=pltpu.CompilerParams(
            collective_id=0, has_side_effects=True, vmem_limit_bytes=61 * 2**20
        ),
    )(
        hidden_in,
        mix_gain[None, :],
        w_value,
        w_gate,
        conv_taps,
        conv_bias[None, :],
        chan_gain[None, :],
        chan_bias[None, :],
        w_back.T,
        feed_gain[None, :],
        w_up,
        w_down,
    )


def solution(mesh):
    placed = (
        P(("rep", "fs"), "tp"),
        P(),
        P("fs", "tp"),
        P("fs", "tp"),
        P(None, "tp"),
        P("tp"),
        P("tp"),
        P("tp"),
        P("tp", "fs"),
        P(),
        P(None, ("fs", "tp")),
        P(("fs", "tp"), None),
    )
    return jax.shard_map(
        shards, mesh=mesh, in_specs=placed, out_specs=P(("rep", "fs"), "tp"), check_vma=False
    )
```

```python
import functools

import jax
import jax.numpy as jnp
from jax import lax
from jax.experimental import pallas as pl
from jax.experimental.pallas import tpu as pltpu
from jax.sharding import PartitionSpec as P

KW = 31
LEN = 128
SIDE = 4
F32 = jnp.float32
BF16 = jnp.bfloat16
UP_PIECES = 4
SPLIT = 0
DOWN_WIDTHS = (256, 256, 256, 128, 128)
DOWN_FIRST = (0, 256, 512, 768, 896)
DOWN_PIECES = len(DOWN_WIDTHS)
PIECES = 2 + UP_PIECES + DOWN_PIECES
UNITS = (1, 0.5) + (4 / UP_PIECES,) * UP_PIECES
UNITS += tuple(width / 256 / (2 if i == SPLIT else 1) for i, width in enumerate(DOWN_WIDTHS))

ORDER = (
    "a0", "a5", "a1", "a6", "a8", "a0", "a10", "a3", "a1", "a7", "a5", "a0", "rmsx", "a3", "a1", "a6", "z10", "z00",
    "a9", "a0", "z01", "a4", "a6", "a10", "a1", "a2", "a3", "a0", "z02", "a6", "vg0", "z11", "a1", "a2", "a4", "a5",
    "a7", "z12", "a6", "a3", "zw0", "vg1", "a4", "y0", "filter", "y1", "a2", "statw", "chan", "a5", "zw1", "bo",
    "a8", "bw", "mixw", "second", "a4", "a2", "secw", "y2", "rms0", "a7", "a5", "a3", "rms1", "hopw0", "a8", "a4",
    "a9", "a2", "forw0", "rmsf0", "upf00", "upf01", "hopw1", "y3", "a7", "up0", "up1", "forw1", "a10", "rmsf1",
    "upf10", "a9", "upf11", "a8", "dF0", "up2", "sb0", "a7", "up3", "dF1", "a9", "a10", "dO0", "sb1", "a8", "dF2",
    "dO1", "sb2", "a9", "dF3", "dO2", "sb3", "a10", "dF4", "dO3", "sb4", "dO4",
)


def kernel(
    x_hbm, mix_gain_hbm, wv_hbm, wg_hbm, taps_hbm, conv_bias_hbm, chan_gain_hbm, chan_bias_hbm, wb_hbm,
    feed_gain_hbm, wu_hbm, wd_hbm,
    out_vmem,
    conv_w, up_w, down_w, x_full, normed, padded, filtered, act, stat_own, stat_got,
    mix_gain, taps, conv_bias, chan_gain, chan_bias, feed_gain,
    second, hidden, part, part_got, own_sum, ret_send, ret_got,
    relay, load_sem, send_sem, recv_sem, z_send, z_recv, pair_send, pair_recv, hop_send, hop_recv, y_send, y_recv,
):
    rows, half = x_hbm.shape
    features = 2 * half
    channels = wv_hbm.shape[1]
    k_rows = wv_hbm.shape[0]
    block = wu_hbm.shape[1]
    sequences = rows // LEN
    part_rows = rows // 2

    core = lax.axis_index("tp")
    other = 1 - core
    place = lax.axis_index("fs")
    z_hi = lax.axis_index("rep")
    x = lax.rem(place, SIDE)
    y = lax.rem(place // SIDE, SIDE)
    z_lo = place // (SIDE * SIDE)
    z = z_hi * 2 + z_lo
    x_next, x_prev = lax.rem(x + 1, SIDE), lax.rem(x + SIDE - 1, SIDE)
    y_next, y_prev = lax.rem(y + 1, SIDE), lax.rem(y + SIDE - 1, SIDE)
    z_next, z_prev = lax.rem(z + 1, 4), lax.rem(z + 3, 4)

    def at_x(xx):
        return {"fs": z_lo * SIDE * SIDE + y * SIDE + xx}

    def at_y(yy):
        return {"fs": z_lo * SIDE * SIDE + yy * SIDE + x}

    def at_z(zz):
        return {"rep": zz // 2, "fs": lax.rem(zz, 2) * SIDE * SIDE + y * SIDE + x}

    partner = {"tp": other}
    mesh_type = pl.DeviceIdType.MESH

    def remote(src, dst, send, recv, device):
        return pltpu.make_async_remote_copy(
            src_ref=src, dst_ref=dst, send_sem=send, recv_sem=recv, device_id=device, device_id_type=mesh_type
        )

    def of(ref, i, n):
        return pl.ds(pl.multiple_of(i * n, n), n)

    conv_row = z_lo * SIDE + y
    loads = [
        pltpu.make_async_copy(wv_hbm, conv_w.at[conv_row, of(0, x, k_rows), 0:channels], load_sem.at[0]),
        pltpu.make_async_copy(wg_hbm, conv_w.at[conv_row, of(0, x, k_rows), channels : 2 * channels], load_sem.at[1]),
        pltpu.make_async_copy(wb_hbm, conv_w.at[conv_row, of(0, x, k_rows), 2 * channels : 3 * channels], load_sem.at[2]),
        pltpu.make_async_copy(wu_hbm, up_w.at[y, :, of(0, x, block)], load_sem.at[3]),
        pltpu.make_async_copy(x_hbm, x_full.at[:, of(0, core, half)], load_sem.at[4]),
    ]
    for index in range(DOWN_PIECES):
        width, first = DOWN_WIDTHS[index], DOWN_FIRST[index]
        for h in range(2):
            size, shift, sem = width, 0, 5
            if index == SPLIT:
                size, sem = width // 2, 12
                shift = z_hi * size
            src = wd_hbm.at[:, pl.ds(pl.multiple_of(h * half + first + shift, 128), size)]
            dst = down_w.at[y, of(0, x, block), pl.ds(pl.multiple_of(2 * first + h * width + shift, 128), size)]
            loads.append(pltpu.make_async_copy(src, dst, load_sem.at[sem]))
    small = [(mix_gain_hbm, mix_gain), (taps_hbm, taps), (conv_bias_hbm, conv_bias)]
    small += [(chan_gain_hbm, chan_gain), (chan_bias_hbm, chan_bias), (feed_gain_hbm, feed_gain)]
    small_loads = [pltpu.make_async_copy(src, dst, load_sem.at[6 + i]) for i, (src, dst) in enumerate(small)]
    for load in loads + small_loads:
        load.start()

    barrier = pltpu.get_barrier_semaphore()
    for device in (at_x(x_next), at_x(x_prev), at_y(y_next), at_y(y_prev), at_z(z_next), at_z(z_prev), partner):
        pl.semaphore_signal(barrier, inc=1, device_id=device, device_id_type=mesh_type)
    with jax.named_scope("barrier"):
        pl.semaphore_wait(barrier, 7)

    def span(first, size, part):
        return pl.ds(first, size) if part is None else pl.ds(first + part * (size // 2), size // 2)

    def conv_piece(first, width):
        def view(what, yy, xx, colour, part):
            cols = span(first + colour * width, width, part)
            if what == "block":
                return conv_w.at[z_lo * SIDE + yy, of(0, xx, k_rows), cols]
            if what == "row":
                return conv_w.at[z_lo * SIDE + yy, :, cols]
            return conv_w.at[pl.ds(z_lo * SIDE, SIDE), of(0, xx, k_rows), cols]

        return view

    def up_piece(index):
        size = features // UP_PIECES // 2

        def view(what, yy, xx, colour, part):
            depth = span((2 * index + colour) * size, size, part)
            if what == "block":
                return up_w.at[yy, depth, of(0, xx, block)]
            if what == "row":
                return up_w.at[yy, depth, :]
            return up_w.at[:, depth, of(0, xx, block)]

        return view

    def split_cols(colour, which):
        width, first = DOWN_WIDTHS[SPLIT], DOWN_FIRST[SPLIT]
        return pl.ds(pl.multiple_of(2 * first + colour * width + which * (width // 2), 128), width // 2)

    def split_send(part):
        rows_of = pl.ds(part * 2, 2)
        for colour, device in ((0, at_z(z_next)), (1, at_z(z_prev))):
            src = down_w.at[rows_of, :, split_cols(colour, z_hi)]
            remote(src, relay.at[colour, rows_of], y_send.at[part], y_recv.at[part], device).start()

    def split_wait(number):
        both = relay.at[:, 0:2]
        pltpu.make_async_copy(both, both, y_recv.at[number]).wait()
        pltpu.make_async_copy(both, both, y_send.at[number]).wait()

    def split_pass(part):
        split_wait(part)
        rows_of = pl.ds(part * 2, 2)
        for colour, device, source in ((0, at_z(z_next), z_prev), (1, at_z(z_prev), z_next)):
            dst = down_w.at[rows_of, :, split_cols(colour, source // 2)]
            remote(relay.at[colour, rows_of], dst, y_send.at[2 + part], y_recv.at[2 + part], device).start()

    def down_piece(index):
        width, first = DOWN_WIDTHS[index], DOWN_FIRST[index]

        def view(what, yy, xx, colour, part):
            cols = pl.ds(2 * first + colour * width, width)
            if index == SPLIT:
                cols = split_cols(colour, z_hi)
            size = block if part is None else block // 2
            rows_of_block = pl.ds(pl.multiple_of(xx * block + (part or 0) * size, size), size)
            if what == "block":
                return down_w.at[yy, rows_of_block, cols]
            if what == "row":
                return down_w.at[yy, span(0, SIDE * block, part), cols]
            return down_w.at[:, rows_of_block, cols]

        return view

    views = [conv_piece(0, channels), conv_piece(2 * channels, channels // 2)]
    views += [up_piece(i) for i in range(UP_PIECES)] + [down_piece(i) for i in range(DOWN_PIECES)]

    def step_copies(piece, step):
        view = views[piece]
        if step == 0:
            own = [("block", y, x, 0, None), ("block", y, x, 1, None)]
            pairs = [(own[0], own[0]), (own[1], own[1])]
        elif step == 1:
            pairs = [
                (("block", y, x_prev, 0, 0), ("block", y, x_next, 0, 1)),
                (("block", y_prev, x, 1, 0), ("block", y_next, x, 1, 1)),
            ]
        elif step == 2:
            pairs = [(("row", y, x, 0, None),) * 2, (("col", y, x, 1, None),) * 2]
        else:
            pairs = [
                (("row", y_prev, x, 0, 0), ("row", y_next, x, 0, 1)),
                (("col", y, x_prev, 1, 0), ("col", y, x_next, 1, 1)),
            ]
        along_x = (at_x(x_next), at_x(x_prev))
        along_y = (at_y(y_next), at_y(y_prev))
        copies = []
        for colour in range(2):
            devices = along_x if (step < 2) == (colour == 0) else along_y
            for way in range(2):
                ref = view(*pairs[colour][way])
                copies.append(remote(ref, ref, send_sem.at[piece], recv_sem.at[piece * 4 + step], devices[way]))
        return copies

    flying = {}

    def z_copies(piece, stage):
        view = views[piece]
        sets = {
            0: [(("row", y, x, 0, None), ("col", y, x, 1, None))],
            1: [
                (("row", y_prev, x, 0, None), ("col", y, x_prev, 1, None)),
                (("row", y_next, x, 0, None), ("col", y, x_next, 1, None)),
            ],
            2: [(("row", lax.rem(y + 2, SIDE), x, 0, None), ("col", y, lax.rem(x + 2, SIDE), 1, None))],
        }[stage]
        copies = []
        for pair in sets:
            for colour in range(2):
                ref = view(*pair[colour])
                copies.append(remote(ref, ref, z_send.at[piece], z_recv.at[piece], at_z((z_next, z_prev)[colour])))
        return copies

    counts = {}

    def advance(piece):
        counts[piece] = counts.get(piece, 0) + 1
        step = 0
        if piece in flying:
            step = flying[piece]
            with jax.named_scope(f"wait_{piece}_{step}"):
                kib = int(4 * UNITS[piece] * 64 * (1, 0.5, 4, 2)[step])
                four = up_w.at[0, 0:kib, :]
                pltpu.make_async_copy(four, four, recv_sem.at[piece * 4 + step]).wait()
                pltpu.make_async_copy(four, four, send_sem.at[piece]).wait()
            step += 1
        if step < 4:
            copies = step_copies(piece, step)
            for copy in copies:
                copy.start()
            flying[piece] = step

    def z_go(piece, stage):
        for copy in z_copies(piece, stage):
            copy.start()

    def z_wait(piece):
        first = 2 * channels * piece
        whole = conv_w.at[pl.ds((1 - z_lo) * SIDE, SIDE), :, pl.ds(first, (2 - piece) * channels)]
        pltpu.make_async_copy(whole, whole, z_recv.at[piece]).wait()
        pltpu.make_async_copy(whole, whole, z_send.at[piece]).wait()

    ups = list(range(2, 2 + UP_PIECES))
    downs = list(range(2 + UP_PIECES, PIECES))

    def rms(src, dst, gain, first, count, step_rows=32, to=0):
        scale = gain[...]

        def body(i, carry):
            at = pl.ds(pl.multiple_of(to + i * step_rows, step_rows), step_rows)
            values = src[pl.ds(pl.multiple_of(first + i * step_rows, step_rows), step_rows), :].astype(F32)
            mean = jnp.sum(values * values, axis=1, keepdims=True) * (1.0 / features)
            dst[at, :] = (values * lax.rsqrt(mean + 1e-6) * scale).astype(BF16)
            return carry

        lax.fori_loop(0, count // step_rows, body, 0, unroll=2)

    mine = of(0, core, half)
    own, foreign = pl.ds(0, rows), pl.ds(rows, rows)
    mix_send, mix_got = part.at[0, 0:rows, :], part_got.at[0:rows, :]
    x_swap = remote(x_hbm, x_full.at[:, mine], pair_send.at[0], pair_recv.at[0], partner)
    stat_swap = remote(stat_own, stat_got, pair_send.at[1], pair_recv.at[1], partner)
    mix_swap = remote(mix_send, mix_got, pair_send.at[2], pair_recv.at[2], partner)
    second_swap = remote(second.at[own, mine], second.at[own, mine], pair_send.at[3], pair_recv.at[3], partner)
    part_rows, strip = rows // 2, rows // 4

    def strip_of(first, k, way):
        return pl.ds(first + k * part_rows + way * strip, strip)

    def home_of(k, way):
        return pl.ds(way * part_rows + k * strip, strip)

    far = [second.at[pl.ds(rows + k * part_rows, part_rows), mine] for k in range(2)]
    foreign_swap = [remote(far[k], far[k], pair_send.at[4 + k], pair_recv.at[4 + k], partner) for k in range(2)]
    hops = [
        remote(
            second.at[home_of(k, way), mine], second.at[strip_of(rows, k, way), mine],
            hop_send.at[k], hop_recv.at[k], at_z((z_next, z_prev)[way]),
        )
        for k in range(2)
        for way in range(2)
    ]

    def first_norm():
        loads[4].wait()
        for load in small_loads:
            load.wait()
        x_swap.wait()
        rms(x_full, normed, mix_gain, 0, rows)
        padded[:, 0:32, :] = jnp.zeros((sequences, 32, channels), F32)

    tile = 256

    def plane_dot(which, cols):
        at = pl.ds(pl.multiple_of(which * half, half), half)
        weights = conv_w[pl.ds(which * SIDE, SIDE), :, cols].reshape(half, tile)
        return jnp.dot(normed[:, at], weights, preferred_element_type=F32)

    def value_gate_own():
        for n in range(2 * channels // tile):
            cols = slice(n * tile, (n + 1) * tile)
            own_sum[:, cols] = plane_dot(z_lo, cols)

    def value_gate_rest():
        for n in range(channels // tile):
            cols = slice(n * tile, (n + 1) * tile)
            gcols = slice(channels + n * tile, channels + (n + 1) * tile)
            value = own_sum[:, cols] + plane_dot(1 - z_lo, cols)
            gate = own_sum[:, gcols] + plane_dot(1 - z_lo, gcols)
            gated = value * jax.nn.sigmoid(gate)
            padded[:, 32 : 32 + LEN, cols] = gated.reshape(sequences, LEN, tile)

    def causal_filter():
        def body(s, carry):
            at = pl.ds(pl.multiple_of(s * LEN, LEN), LEN)
            first = jnp.zeros((LEN, 128), F32)
            square = jnp.zeros((LEN, 128), F32)
            for lane in range(channels // 128):
                cols = slice(lane * 128, (lane + 1) * 128)
                slab = padded[s, :, cols]
                total = jnp.broadcast_to(conv_bias[:, cols], (LEN, 128))
                for shift in range(8):
                    acc = None
                    for q in range(5):
                        k = 8 * q + shift - 2
                        if 0 <= k < KW:
                            tall = LEN + (8 if shift else 0)
                            term = taps[k : k + 1, cols] * slab[8 * q : 8 * q + tall]
                            acc = term if acc is None else acc + term
                    total = total + acc[shift : shift + LEN]
                filtered[at, cols] = total
                first = first + total
                square = square + total * total
            stat_own[0, at, :] = first
            stat_own[1, at, :] = square
            return carry

        lax.fori_loop(0, sequences, body, 0)
        stat_swap.start()

    def channel_norm():
        def body(i, carry):
            at = pl.ds(pl.multiple_of(i * 64, 64), 64)
            scale = 1.0 / (2 * channels)
            mean = jnp.sum(stat_own[0, at, :] + stat_got[0, at, :], axis=1, keepdims=True) * scale
            power = jnp.sum(stat_own[1, at, :] + stat_got[1, at, :], axis=1, keepdims=True) * scale
            spread = lax.rsqrt(power - mean * mean + 1e-5)
            centred = (filtered[at, :] - mean) * spread * chan_gain[...] + chan_bias[...]
            act[at, :] = (centred * jax.nn.sigmoid(centred)).astype(BF16)
            return carry

        lax.fori_loop(0, rows // 64, body, 0)

    def back_half(which):
        weights = conv_w[pl.ds(which * SIDE, SIDE), :, 2 * channels : 3 * channels].reshape(half, channels)
        return lax.dot_general(act[...], weights, (((1,), (1,)), ((), ())), preferred_element_type=F32)

    def back_other():
        mix_send[...] = back_half(other).astype(BF16)
        mix_swap.start()

    def back_own():
        own_sum[...] = back_half(core)

    def residual():
        mixed = own_sum[...].astype(BF16).astype(F32) + mix_got[...].astype(F32)
        second[own, mine] = (x_full[:, mine].astype(F32) + mixed).astype(BF16)
        for hop in hops:
            hop.start()
        second_swap.start()

    def up(source, first, begin, end):
        at = pl.ds(first, source.shape[0])

        def body(i, carry):
            product = jnp.dot(source[...], up_w[i], preferred_element_type=F32)
            positive = jnp.maximum(product, 0.0)
            hidden[at, pl.ds(pl.multiple_of(i * SIDE * block, SIDE * block), SIDE * block)] = (positive * positive).astype(BF16)
            return carry

        lax.fori_loop(begin, end, body, 0)

    def arrived(k):
        pltpu.make_async_copy(far[k], far[k], hop_recv.at[k]).wait()
        pltpu.make_async_copy(far[k], far[k], hop_send.at[k]).wait()
        foreign_swap[k].start()

    def far_norm(k):
        rms(second, x_full, feed_gain, rows + k * part_rows, part_rows, to=k * part_rows)

    def far_up(k, begin):
        up(x_full.at[pl.ds(k * part_rows, part_rows), :], rows + k * part_rows, begin, begin + SIDE // 2)

    swaps = {}

    def down(index, number):
        width, first = DOWN_WIDTHS[index], DOWN_FIRST[index]
        cols = pl.ds(first, width)
        depth = SIDE * SIDE * block
        at = (foreign, own)[number]
        many = 1 if width >= 256 else 2
        if index == SPLIT and number == 0:
            split_wait(2)
            split_wait(3)

        def body(i, carry):
            chunk = pl.ds(pl.multiple_of(at.start + i * (rows // many), rows // many), rows // many)
            weights = down_w[:, :, pl.ds(2 * first, 2 * width)].reshape(depth, 2 * width)
            product = jnp.dot(hidden[chunk, :], weights, preferred_element_type=F32).astype(BF16)
            part[0, chunk, cols] = product[:, :width]
            part[1, chunk, cols] = product[:, width:]
            return carry

        lax.fori_loop(0, many, body, 0)
        sem = pair_send.at[6 + number * (1 + index)]
        swap = remote(part.at[other, at, cols], part_got.at[at, cols], sem, pair_recv.at[6 + 2 * index + number], partner)
        swap.start()
        swaps[index, number] = swap

    def send_back(index):
        width, first = DOWN_WIDTHS[index], DOWN_FIRST[index]
        cols = pl.ds(first, width)
        swaps[index, 0].wait()
        ret_send[:, cols] = (part[core, foreign, cols].astype(F32) + part_got[foreign, cols].astype(F32)).astype(BF16)
        for k in range(2):
            for way, device in ((0, at_z(z_prev)), (1, at_z(z_next))):
                src, dst = ret_send.at[strip_of(0, k, way), cols], ret_got.at[home_of(k, way), cols]
                remote(src, dst, hop_send.at[2 + index], hop_recv.at[2 + index], device).start()

    def finish(index):
        width, first = DOWN_WIDTHS[index], DOWN_FIRST[index]
        cols = pl.ds(first, width)
        swaps[index, 1].wait()
        both = ret_got.at[:, cols]
        pltpu.make_async_copy(both, both, hop_recv.at[2 + index]).wait()
        pltpu.make_async_copy(both, both, hop_send.at[2 + index]).wait()
        there = pl.ds(pl.multiple_of(core * half + first, 128), width)
        total = second[own, there].astype(F32) + part[core, own, cols].astype(F32) + part_got[own, cols].astype(F32)
        out_vmem[:, cols] = (total + ret_got[:, cols].astype(F32)).astype(BF16)

    actions = dict(
        rmsx=first_norm,
        vg0=value_gate_own,
        zw0=lambda: z_wait(0),
        vg1=value_gate_rest,
        filter=causal_filter,
        statw=stat_swap.wait,
        chan=channel_norm,
        zw1=lambda: z_wait(1),
        bo=back_other,
        bw=back_own,
        mixw=mix_swap.wait,
        second=residual,
        secw=second_swap.wait,
        rms0=lambda: rms(second, normed, feed_gain, 0, part_rows),
        rms1=lambda: rms(second, normed, feed_gain, part_rows, part_rows, to=part_rows),
        hopw0=lambda: arrived(0),
        hopw1=lambda: arrived(1),
        forw0=foreign_swap[0].wait,
        forw1=foreign_swap[1].wait,
        rmsf0=lambda: far_norm(0),
        rmsf1=lambda: far_norm(1),
    )
    for index in range(SIDE):
        actions[f"up{index}"] = functools.partial(up, normed, 0, index, index + 1)
    for k in range(2):
        for index in range(2):
            actions[f"upf{k}{index}"] = functools.partial(far_up, k, 2 * index)
    for index in range(DOWN_PIECES):
        actions[f"dF{index}"] = functools.partial(down, index, 0)
        actions[f"dO{index}"] = functools.partial(down, index, 1)
        actions[f"sb{index}"] = functools.partial(send_back, index)

    first_load = {0: (0, 1), 1: (2,)}
    first_load.update({piece: (3,) for piece in ups})
    first_load.update({piece: (6 if i == SPLIT else 5,) for i, piece in enumerate(downs)})
    split_width = DOWN_WIDTHS[SPLIT]
    most = down_w.at[y, of(0, x, block), 0 : features - 2 * split_width]
    few = down_w.at[y, of(0, x, block), 0:split_width]
    loads[5:] = [pltpu.make_async_copy(most, most, load_sem.at[5]), pltpu.make_async_copy(few, few, load_sem.at[12])]
    loaded = set()

    x_swap.start()
    for name in ORDER:
        if name[0] == "a" and name[1:].isdigit():
            piece = int(name[1:])
            for number in first_load[piece]:
                if number not in loaded:
                    loads[number].wait()
                    loaded.add(number)
            advance(piece)
        elif name[0] == "y":
            number = int(name[1:])
            with jax.named_scope(name):
                (split_send if number < 2 else split_pass)(number % 2)
        elif name[0] == "z" and name[1:].isdigit():
            z_go(int(name[1]), int(name[2]))
        else:
            with jax.named_scope(name):
                actions[name]()

    for index in range(DOWN_PIECES):
        with jax.named_scope(f"finish{index}"):
            finish(index)
    assert all(counts[piece] == 5 for piece in range(PIECES)), counts


def shards(
    hidden_in, mix_gain, w_value, w_gate, conv_taps, conv_bias, chan_gain, chan_bias, w_back, feed_gain, w_up, w_down
):
    rows, half = hidden_in.shape
    features = 2 * half
    channels = w_value.shape[1]
    block = w_up.shape[1]
    plane = SIDE * SIDE
    sequences = rows // LEN
    vmem = pl.BlockSpec(memory_space=pltpu.VMEM)
    hbm = pl.BlockSpec(memory_space=pl.ANY)
    dma = pltpu.SemaphoreType.DMA
    scratch = [
        pltpu.VMEM((2 * SIDE, SIDE * w_value.shape[0], 3 * channels), BF16),
        pltpu.VMEM((SIDE, features, SIDE * block), BF16),
        pltpu.VMEM((SIDE, SIDE * block, features), BF16),
        pltpu.VMEM((rows, features), BF16),
        pltpu.VMEM((rows, features), BF16),
        pltpu.VMEM((sequences, 32 + LEN, channels), F32),
        pltpu.VMEM((rows, channels), F32),
        pltpu.VMEM((rows, channels), BF16),
        pltpu.VMEM((2, rows, 128), F32),
        pltpu.VMEM((2, rows, 128), F32),
        pltpu.VMEM((1, features), F32),
        pltpu.VMEM(conv_taps.shape, F32),
        pltpu.VMEM((1, channels), F32),
        pltpu.VMEM((1, channels), F32),
        pltpu.VMEM((1, channels), F32),
        pltpu.VMEM((1, features), F32),
        pltpu.VMEM((2 * rows, features), BF16),
        pltpu.VMEM((2 * rows, plane * block), BF16),
        pltpu.VMEM((2, 2 * rows, half), BF16),
        pltpu.VMEM((2 * rows, half), BF16),
        pltpu.VMEM((rows, half), F32),
        pltpu.VMEM((rows, half), BF16),
        pltpu.VMEM((rows, half), BF16),
        pltpu.VMEM((2, SIDE, SIDE * block, DOWN_WIDTHS[SPLIT] // 2), BF16),
        dma((13,)),
        dma((PIECES,)),
        dma((PIECES * 4,)),
        dma((2,)),
        dma((2,)),
        dma((7 + DOWN_PIECES,)),
        dma((6 + 2 * DOWN_PIECES,)),
        dma((2 + DOWN_PIECES,)),
        dma((2 + DOWN_PIECES,)),
        dma((4,)),
        dma((4,)),
    ]
    return pl.pallas_call(
        kernel,
        out_shape=pltpu.VMEM((rows, half), BF16),
        in_specs=[hbm] * 12,
        out_specs=vmem,
        scratch_shapes=scratch,
        compiler_params=pltpu.CompilerParams(
            collective_id=0, has_side_effects=True, vmem_limit_bytes=61 * 2**20
        ),
    )(
        hidden_in,
        mix_gain[None, :],
        w_value,
        w_gate,
        conv_taps,
        conv_bias[None, :],
        chan_gain[None, :],
        chan_bias[None, :],
        w_back.T,
        feed_gain[None, :],
        w_up,
        w_down,
    )


def solution(mesh):
    placed = (
        P(("rep", "fs"), "tp"),
        P(),
        P("fs", "tp"),
        P("fs", "tp"),
        P(None, "tp"),
        P("tp"),
        P("tp"),
        P("tp"),
        P("tp", "fs"),
        P(),
        P(None, ("fs", "tp")),
        P(("fs", "tp"), None),
    )
    return jax.shard_map(
        shards, mesh=mesh, in_specs=placed, out_specs=P(("rep", "fs"), "tp"), check_vma=False
    )
```
